32 devices in a mesh: sp: 8 (over z, x), tp: 4 (over y, core).
Axes of the slice: x: 2, y: 2, z: 4, core: 2. Of those that a mesh axis runs over, the one named last changes fastest.
Arguments:
- outer_gate: bfloat16 [2048, 2048], P('sp', 'tp'), may hold values from -6 to 6
- inner_gate: bfloat16 [2048, 2048], P('sp', 'tp'), may hold values from -6 to 6
- conv_input: bfloat16 [2048, 2048], P('sp', 'tp'), may hold values from -6 to 6
- conv_weight: bfloat16 [3, 2048], P(None, 'tp'), may hold values from -3.5 to 3.5
- doc_ids: int32 [2048], P('sp'), may hold values from 0 to 3, as said below
- output_weight: bfloat16 [2048, 4096], P(None, 'tp'), may hold values from -0.125 to 0.125
- residual: bfloat16 [2048, 4096], P('sp', 'tp'), as said below
- norm_gain: bfloat16 [4096], P('tp'), may hold values from 0.099609375 to 1.8984375
- expert_ids: int32 [2048, 2], P('sp'), may hold values from 0 to 7, all different within a row; in each aligned block of 256 rows (0 to 255, 256 to 511, ...) at most 128 rows name the same one
- group_weight: float32 [2048], P('sp'), may hold values from 0.25 to 1
- expert_weight: float32 [2048, 2], P('sp'), may hold values from 0.05 to 1
- gate_weight: bfloat16 [8, 4096, 2048], P('sp', None, 'tp'), may hold values from -0.09375 to 0.09375
- up_weight: bfloat16 [8, 4096, 2048], P('sp', None, 'tp'), may hold values from -0.09375 to 0.09375
- down_weight: bfloat16 [8, 2048, 4096], P('sp', None, 'tp'), may hold values from -0.125 to 0.125
Outputs:
- layer_out: bfloat16 [2048, 4096], P('sp', 'tp')
The draws below stay inside these ranges and needn't reach their ends.
Inputs may be any that keep to these rules, and one draw needn't show every extreme that they name: `expert_ids`: within the 256 rows of one index of sp no expert is named more than 128 times, a bound that some block reaches; the two experts of a row differ. `doc_ids`: never falling along positions, rising by one at each document's start; every document has 256 to 768 positions, and one exactly 768. `residual`: Columns' scales are of order one to ten.
All inputs are finite; a program needn't handle non-finite values.
Results may differ from the reference program's by a relative error of at most 0.009.
Values may be sent and summed in bfloat16 or wider, within the bound.
A program may use at most 64 MiB of HBM per device.

```python
import math
import jax
import jax.numpy as jnp
import numpy as np
from jax import lax

D = 4096
BRANCH = 2048
FFN = 2048
TAPS = 3
TOK = 256
TOKENS = 2048
EXPERTS = 8
CAP = 128
N_SP = 8


def draw_residual(key, part):
    column_scale = 10.0 ** (jnp.arange(D, dtype=jnp.float32) / D)
    base = jax.random.normal(key, (TOKENS, D), jnp.float32)
    return (base * column_scale * 0.5).astype(jnp.bfloat16)


def draw_doc_ids(key, part):
    bound_total = N_SP // 2 - 1
    jitters = jax.random.randint(jax.random.fold_in(key, 11), (bound_total,), 0, TOK, dtype=jnp.int32)
    longest = jax.random.randint(jax.random.fold_in(key, 13), (), 0, bound_total, dtype=jnp.int32)
    marker = jnp.arange(bound_total, dtype=jnp.int32)
    jitters = jnp.where(marker == longest - 1, 0, jitters)
    jitters = jnp.where(marker == longest, TOK, jitters)
    starts = (marker + 1) * (2 * TOK) + jitters
    positions = jnp.arange(TOKENS, dtype=jnp.int32)
    return jnp.sum((positions[:, None] >= starts[None, :]).astype(jnp.int32), axis=1).astype(jnp.int32)


def level_of(rng, extent, pieces, least, largest):
    loudness, own = 1.0, jax.random.fold_in(rng, 6)
    for axis_at, blocks in pieces:
        heights = jnp.exp(jax.random.uniform(jax.random.fold_in(own, axis_at), (blocks,), jnp.float32, least / len(pieces), largest / len(pieces)))
        loudness = loudness * jnp.repeat(heights, extent[axis_at] // blocks).reshape([-1 if axis == axis_at else 1 for axis in range(len(extent))])
    return loudness


def deal_out(stream_key, own, number, rows, amount, top, bound, lean):
    sequence = jax.random.permutation(stream_key, amount)
    heavy_load, ordinary = shares(amount, rows * top, bound, lean, True), shares(amount, rows * top, bound, lean, False)
    places = jnp.arange(amount)

    def named(tallies, turn):
        used = int((tallies > 0).sum())
        fixed = max(1, used // 4)
        moved = fixed + (places - fixed + turn * (used - fixed)) % max(1, amount - fixed)
        return jnp.zeros((amount,), jnp.int32).at[sequence[jnp.where(places < fixed, places, moved)]].set(jnp.asarray(tallies, jnp.int32))

    tallies = jnp.where(number % 4 == 0, named(heavy_load, number // 4), named(ordinary, number - number // 4 - 1))
    mixed = jax.random.permutation(jax.random.fold_in(own, 3), amount)
    source_of, sink = mixed[0:amount // 2 * 2:2], mixed[1:amount // 2 * 2:2]
    margin = jnp.minimum(tallies[source_of] - 1, bound - tallies[sink]) // 2
    margin = jnp.where((source_of == sequence[0]) | (sink == sequence[0]) | (tallies[sink] == 0), 0, jnp.maximum(margin, 0))
    moved = jax.random.randint(jax.random.fold_in(own, 4), (amount // 2,), 0, 1 << 20) % (margin + 1)
    tallies = tallies.at[source_of].add(-moved).at[sink].add(moved)
    items = jnp.searchsorted(jnp.cumsum(tallies), jnp.arange(rows * top), side="right").astype(jnp.int32)
    grid = items.reshape(top, rows).T
    grid = grid[jax.random.permutation(jax.random.fold_in(own, 1), rows)]
    turn = jax.random.randint(jax.random.fold_in(own, 2), (rows, 1), 0, top)
    return jnp.take_along_axis(grid, (jnp.arange(top)[None, :] + turn) % top, axis=1)


def shares(count, total, reach, skew, full):
    portions = [(1 << 20) // math.isqrt(rank ** skew) + 1 for rank in range(1, count + 1)]
    largest = reach if full else min(reach, max(-(-total // count), total * portions[0] // sum(portions)))
    least = 1 if total - largest >= count - 1 else 0
    counts, rest = [largest] + [least] * (count - 1), total - largest - least * (count - 1)
    while rest > 0:
        candidates = [i for i in range(1, count) if counts[i] < largest] or [i for i in range(1, count) if counts[i] < reach]
        whole, remaining = sum([portions[i] for i in candidates]), rest
        for i in candidates:
            more = min(reach - counts[i], max(1, remaining * portions[i] // whole), rest)
            counts[i] = counts[i] + more
            rest = rest - more
    return np.array(counts)


def centred(rng, extent, width, limit, cuts=(), kind=jnp.bfloat16):
    values = jax.random.normal(rng, extent, jnp.float32) * width
    if len(cuts) > 0:
        values = level_of(rng, extent, cuts, -0.22, 0.18) * values
    return jnp.clip(values, min=-limit, max=limit).astype(kind)


def setup_inputs(seed: int = 0) -> dict:
    key_of = jax.random.split(jax.random.key(seed), 15)
    outer_gate = centred(key_of[0], (TOKENS, BRANCH), 1.0, 6.0, ((0, 8), (1, 4)))
    inner_gate = centred(key_of[1], (TOKENS, BRANCH), 1.0, 6.0, ((0, 8), (1, 4)))
    conv_input = centred(key_of[2], (TOKENS, BRANCH), 1.0, 6.0, ((0, 8), (1, 4)))
    conv_weight = centred(key_of[3], (TAPS, BRANCH), TAPS ** -0.5, 3.5, ((1, 4),))
    doc_ids = draw_doc_ids(jax.random.fold_in(key_of[14], 71), 0)
    output_weight = centred(key_of[5], (BRANCH, D), BRANCH ** -0.5, 0.125, ((1, 4),))
    residual = draw_residual(jax.random.fold_in(key_of[14], 71), 0)
    norm_gain = jnp.clip(1.0 + 0.18 * jax.random.normal(key_of[7], (D,), jnp.float32), 0.099609375, 1.8984375).astype(jnp.bfloat16)
    expert_ids_keys = jax.random.split(jax.random.fold_in(key_of[8], 1), TOKENS // TOK)
    expert_ids_turns = jax.random.permutation(jax.random.fold_in(key_of[8], 3), TOKENS // TOK)
    expert_ids = jax.vmap(lambda own, number: deal_out(jax.random.fold_in(key_of[8], 2), own, number, TOK, EXPERTS, 2, CAP, 2))(expert_ids_keys, expert_ids_turns).reshape((TOKENS, 2))
    group_weight = jnp.clip(0.25 + 0.75 * jax.random.uniform(key_of[9], (TOKENS,), jnp.float32) ** level_of(key_of[9], (TOKENS,), ((0, 8),), -0.2, 0.2), 0.25, 1.0)
    expert_weight = jnp.clip(jnp.exp(math.log(1.0) - 2.9957323 * jax.random.uniform(key_of[10], (TOKENS, 2), jnp.float32) ** level_of(key_of[10], (TOKENS, 2), ((0, 8),), -0.2, 0.2)), 0.05, 1.0)
    gate_weight = centred(key_of[11], (EXPERTS, D, FFN), D ** -0.5, 0.09375, ((0, 8), (2, 4)))
    up_weight = centred(key_of[12], (EXPERTS, D, FFN), D ** -0.5, 0.09375, ((0, 8), (2, 4)))
    down_weight = centred(key_of[13], (EXPERTS, FFN, D), FFN ** -0.5, 0.125, ((0, 8), (2, 4)))
    return {"outer_gate": outer_gate, "inner_gate": inner_gate, "conv_input": conv_input, "conv_weight": conv_weight, "doc_ids": doc_ids, "output_weight": output_weight, "residual": residual, "norm_gain": norm_gain, "expert_ids": expert_ids, "group_weight": group_weight, "expert_weight": expert_weight, "gate_weight": gate_weight, "up_weight": up_weight, "down_weight": down_weight}


EPS = 1e-06

def reference(outer_gate, inner_gate, conv_input, conv_weight, doc_ids, output_weight, residual, norm_gain, expert_ids, group_weight, expert_weight, gate_weight, up_weight, down_weight):
    products = inner_gate.astype(jnp.float32) * conv_input.astype(jnp.float32)
    taps = conv_weight.astype(jnp.float32)
    conv = taps[2] * products
    for shift_by in (1, 2):
        earlier = jnp.pad(products, ((shift_by, 0), (0, 0)))[:-shift_by]
        earlier_docs = jnp.pad(doc_ids, (shift_by, 0), constant_values=-1)[:-shift_by]
        same_doc = (earlier_docs == doc_ids)[:, None]
        conv = conv + jnp.where(same_doc, taps[2 - shift_by] * earlier, 0.0)
    branch = (outer_gate.astype(jnp.float32) * conv).astype(jnp.bfloat16)
    branch_sum = jnp.dot(branch, output_weight, preferred_element_type=jnp.float32)
    resid = (residual.astype(jnp.float32) + branch_sum).astype(jnp.bfloat16)
    resid_wide = resid.astype(jnp.float32)
    scale = lax.rsqrt(lax.optimization_barrier(jnp.mean(resid_wide * resid_wide, axis=1, keepdims=True)) + EPS)
    normed = (resid_wide * scale * norm_gain.astype(jnp.float32)).astype(jnp.bfloat16)
    mix_weight = group_weight[:, None] * expert_weight / lax.optimization_barrier(jnp.sum(expert_weight, axis=1, keepdims=True))
    flat_experts = expert_ids.reshape(N_SP, 2 * TOK)
    onehot = (flat_experts[:, :, None] == jnp.arange(EXPERTS, dtype=jnp.int32)[None, None, :]).astype(jnp.int32)
    slot_rank = lax.optimization_barrier(jnp.sum((jnp.cumsum(onehot, axis=1) - onehot) * onehot, axis=2)).astype(jnp.int32)
    slot_index = flat_experts * CAP + slot_rank
    token_of = jnp.broadcast_to(jnp.arange(2 * TOK, dtype=jnp.int32) // 2, slot_index.shape)
    group_index = jnp.arange(N_SP, dtype=jnp.int32)[:, None]
    token_table = jnp.full((N_SP, EXPERTS * CAP), TOK, jnp.int32).at[group_index, slot_index].set(token_of)
    token_table = token_table.reshape(N_SP, EXPERTS, CAP)
    grouped = jnp.concatenate([normed.reshape(N_SP, TOK, D), jnp.zeros((N_SP, 1, D), jnp.bfloat16)], axis=1)

    def one_expert(expert):
        chosen = lax.dynamic_index_in_dim(token_table, expert, 1, keepdims=False)
        routed = grouped[group_index, chosen].reshape(N_SP * CAP, D)
        gate_val = jnp.dot(routed, gate_weight[expert], preferred_element_type=jnp.float32)
        up_val = jnp.dot(routed, up_weight[expert], preferred_element_type=jnp.float32)
        hidden = (jax.nn.silu(gate_val) * up_val).astype(jnp.bfloat16)
        result = jnp.dot(hidden, down_weight[expert], preferred_element_type=jnp.float32).astype(jnp.bfloat16)
        return result.reshape(N_SP, CAP, D)
    expert_out = lax.map(one_expert, jnp.arange(EXPERTS, dtype=jnp.int32))
    picked = expert_out[flat_experts, group_index, slot_rank].reshape(TOKENS, 2, D).astype(jnp.float32)
    routed_sum = lax.optimization_barrier(jnp.sum(picked * mix_weight[:, :, None], axis=1))
    return (resid_wide + routed_sum).astype(jnp.bfloat16)
```

```python
import functools

import jax
import jax.numpy as jnp
from jax import lax
from jax.experimental import pallas as pl
from jax.experimental.pallas import tpu as pltpu
from jax.sharding import PartitionSpec as P

EPS = 1e-06
MESH = pl.DeviceIdType.MESH


def remote(src, dst, send_sem, recv_sem, device):
    return pltpu.make_async_remote_copy(
        src_ref=src,
        dst_ref=dst,
        send_sem=send_sem,
        recv_sem=recv_sem,
        device_id=device,
        device_id_type=MESH,
    )


def expert_kernel(
    n,
    tp,
    across,
    outer_ref,
    inner_ref,
    conv_ref,
    taps_ref,
    docs_ref,
    residual_ref,
    gain_ref,
    ids_ref,
    mix_ref,
    proj_hbm,
    gate_hbm,
    up_hbm,
    down_hbm,
    result_ref,
    tokens,
    slots_out,
    ret_ref,
    branch,
    proj_w,
    acc,
    resid,
    squares,
    key_col,
    key_rows,
    mix_col,
    halo_inner,
    halo_conv,
    halo_docs,
    piece,
    hid,
    eo,
    gate_w,
    up_w,
    down_w,
    w_sem,
    k_send,
    k_recv,
    a_send,
    a_recv,
    x_send,
    x_recv,
    y_send,
    y_recv,
    p_send,
    p_recv,
    hy_send,
    hy_recv,
    hp_send,
    hp_recv,
    r_send,
    r_recv,
    h_send,
    h_recv,
    by_send,
    by_recv,
    bp_send,
    bp_recv,
    s_send,
    s_recv,
):
    me = lax.axis_index("sp")
    t = lax.axis_index("tp")
    chips = tp // 2
    y, core = lax.div(t, 2), lax.rem(t, 2)
    partner = t + 1 - 2 * core
    cap, cols = ret_ref.shape[1], ret_ref.shape[2]
    ffn_local = gate_w.shape[1]
    depth, group_rows = hid.shape[0], hid.shape[1]
    z, x = lax.div(me, across), lax.rem(me, across)
    chunks = a_recv.shape[1]
    key_count = key_rows.shape[1]

    near = jnp.minimum(z, depth - 1 - z)
    low = 2 * z < depth

    def group_z(g):
        if g == 0:
            return z
        step = (g + 1) // 2
        outward = step if g % 2 else -step
        close = jnp.where(low, z + outward, z - outward)
        far = jnp.where(low, g, depth - 1 - g)
        return jnp.where(g <= 2 * near, close, far)

    def column(index, width):
        return pl.ds(pl.multiple_of(index * width, 128), width)

    def chip_at(delta):
        return lax.rem(y + delta + chips, chips) * 2 + core

    weight_copies = [
        pltpu.make_async_copy(source, target, w_sem.at[i])
        for i, (source, target) in enumerate(
            (
                (gate_hbm.at[0], gate_w),
                (up_hbm.at[0], up_w),
                (down_hbm.at[0], down_w),
                (proj_hbm, proj_w),
            )
        )
    ]
    for i in (3, 0, 1, 2):
        weight_copies[i].start()

    barrier = pltpu.get_barrier_semaphore()
    for k in range(1, n):
        pl.semaphore_signal(
            barrier, inc=1, device_id=(lax.rem(me + k, n), t), device_id_type=MESH
        )
    for d in range(1, tp):
        pl.semaphore_signal(
            barrier, inc=1, device_id=(me, lax.rem(t + d, tp)), device_id_type=MESH
        )
    pl.semaphore_wait(barrier, n - 1 + tp - 1)

    sends = []
    arrivals = []
    row_count = residual_ref.shape[0]
    wide = branch.shape[1] // tp

    halos = []
    following = (lax.rem(me + 1, n), t)
    for i, (source, target) in enumerate(
        (
            (inner_ref.at[pl.ds(row_count - 16, 16)], halo_inner),
            (conv_ref.at[pl.ds(row_count - 16, 16)], halo_conv),
            (docs_ref.at[pl.ds(row_count - 8, 8)], halo_docs),
        )
    ):
        copy = remote(source, target, h_send.at[i], h_recv.at[i], following)
        copy.start()
        halos.append(copy)
        sends.append(copy)

    lanes = lax.broadcasted_iota(jnp.int32, (row_count, 128), 1)
    first_id, second_id = ids_ref[:, 0:1], ids_ref[:, 1:2]
    is_first, is_second = lanes == first_id, lanes == second_id
    mix_col[...] = jnp.where(is_first, mix_ref[:, 0:1], 0.0) + jnp.where(
        is_second, mix_ref[:, 1:2], 0.0
    )
    member = jnp.where(is_first, 1.0, 0.0) + jnp.where(is_second, 1.0, 0.0)
    earlier = jnp.where(
        lax.broadcasted_iota(jnp.int32, (row_count, row_count), 1)
        < lax.broadcasted_iota(jnp.int32, (row_count, row_count), 0),
        1.0,
        0.0,
    ).astype(jnp.bfloat16)
    ranks = jnp.dot(earlier, member.astype(jnp.bfloat16), preferred_element_type=jnp.float32)
    keys = jnp.where(member > 0.5, ranks, -1.0)
    key_col[...] = keys
    key_rows[z] = keys.T[0:key_count]
    for d in range(1, depth):
        copy = remote(
            key_rows.at[z],
            key_rows.at[z],
            k_send.at[d],
            k_recv.at[z],
            (lax.rem(z + d, depth) * across + x, t),
        )
        copy.start()
        sends.append(copy)

    for copy in halos:
        copy.wait_recv()
    row_at = lax.broadcasted_iota(jnp.int32, (row_count, 1), 0)
    own_docs = docs_ref[:, 0:1]
    halo_ids = jnp.where(me > 0, halo_docs[...], -1.0)[:, 0:1]
    docs_one = jnp.where(row_at == 0, halo_ids[7:8], pltpu.roll(docs_ref[...], 1, 0)[:, 0:1])
    docs_two = jnp.where(
        row_at == 0,
        halo_ids[6:7],
        jnp.where(row_at == 1, halo_ids[7:8], pltpu.roll(docs_ref[...], 2, 0)[:, 0:1]),
    )
    same_one, same_two = docs_one == own_docs, docs_two == own_docs

    def conv_tile(j, carry):
        at = pl.ds(pl.multiple_of(j * 128, 128), 128)
        products = inner_ref[:, at].astype(jnp.float32) * conv_ref[:, at].astype(jnp.float32)
        before = halo_inner[:, at].astype(jnp.float32) * halo_conv[:, at].astype(jnp.float32)
        one = jnp.where(row_at == 0, before[15:16], pltpu.roll(products, 1, 0))
        two = jnp.where(
            row_at == 0,
            before[14:15],
            jnp.where(row_at == 1, before[15:16], pltpu.roll(products, 2, 0)),
        )
        taps = taps_ref[:, at].astype(jnp.float32)
        conv = taps[2:3] * products
        conv = conv + jnp.where(same_one, taps[1:2] * one, 0.0)
        conv = conv + jnp.where(same_two, taps[0:1] * two, 0.0)
        value = (outer_ref[:, at].astype(jnp.float32) * conv).astype(jnp.bfloat16)
        branch[:, pl.ds(pl.multiple_of(t * wide + j * 128, 128), 128)] = value
        return carry

    lax.fori_loop(0, wide // 128, conv_tile, 0)

    def branch_region(index):
        return branch.at[:, column(index, wide)]

    region = branch_region(t)
    for d in range(1, chips):
        copy = remote(region, region, by_send.at[d], by_recv.at[d], (me, chip_at(d)))
        copy.start()
        sends.append(copy)
    copy = remote(region, region, bp_send.at[0], bp_recv.at[0], (me, partner))
    copy.start()
    sends.append(copy)
    weight_copies[3].wait()

    def project(index, first=False):
        step = min(256, cols)

        def tile(j, carry):
            at = pl.ds(pl.multiple_of(j * step, 128), step)
            rows = pl.ds(pl.multiple_of(index * wide, 128), wide)
            value = jnp.dot(
                branch[:, column(index, wide)], proj_w[rows, at], preferred_element_type=jnp.float32
            )
            acc[:, at] = value if first else acc[:, at] + value
            return carry

        lax.fori_loop(0, cols // step, tile, 0)

    project(t, True)
    other = branch_region(partner)
    remote(other, other, bp_send.at[0], bp_recv.at[0], (me, partner)).wait_recv()
    project(partner)
    for d in range(1, chips):
        source = chip_at(-d)
        region = branch_region(source)
        remote(region, region, by_send.at[d], by_recv.at[d], (me, partner)).wait_recv()
        copy = remote(region, region, bp_send.at[d], bp_recv.at[d], (me, partner))
        copy.start()
        sends.append(copy)
        project(source)
    for d in range(1, chips):
        source = chip_at(-d) + partner - t
        region = branch_region(source)
        remote(region, region, bp_send.at[d], bp_recv.at[d], (me, partner)).wait_recv()
        project(source)

    def resid_tile(j, total):
        at = pl.ds(pl.multiple_of(j * 128, 128), 128)
        value = (residual_ref[:, at].astype(jnp.float32) + acc[:, at]).astype(jnp.bfloat16)
        resid[:, at] = value
        value = value.astype(jnp.float32)
        return total + value * value

    total = lax.fori_loop(
        0, cols // 128, resid_tile, jnp.zeros((row_count, 128), jnp.float32)
    )
    squares[t] = jnp.broadcast_to(
        jnp.sum(total.T, axis=0, keepdims=True), (8, row_count)
    )
    for d in range(1, tp):
        copy = remote(
            squares.at[t], squares.at[t], s_send.at[d], s_recv.at[d], (me, lax.rem(t + d, tp))
        )
        copy.start()
        sends.append(copy)
    for d in range(1, tp):
        source = lax.rem(t + tp - d, tp)
        remote(
            squares.at[source], squares.at[source], s_send.at[d], s_recv.at[d], (me, source)
        ).wait_recv()
    total_sq = jnp.sum(squares[...], axis=0)[0:1]
    scale_row = lax.rsqrt(total_sq / (tp * cols) + EPS)
    scale = jnp.broadcast_to(scale_row, (128, row_count)).T

    def norm_tile(j, carry):
        at = pl.ds(pl.multiple_of(j * 128, 128), 128)
        value = resid[:, at].astype(jnp.float32) * scale * gain_ref[:, at].astype(jnp.float32)
        tokens[z, :, at] = value.astype(jnp.bfloat16)
        return carry

    lax.fori_loop(0, cols // 128, norm_tile, 0)

    chunk = cols // chunks
    guarded = []

    def token_region(index, c):
        return tokens.at[index, :, pl.ds(c * chunk, chunk)]

    def pass_on(index, c, sem, target):
        inside = (target >= 0) & (target < depth)
        copy = remote(
            token_region(index, c),
            token_region(index, c),
            sem,
            a_recv.at[index, c],
            (target * across + x, t),
        )

        @pl.when(inside)
        def _():
            copy.start()

        return inside, copy

    for c in range(chunks):
        guarded.append(pass_on(z, c, a_send.at[0, c], z + 1))
        guarded.append(pass_on(z, c, a_send.at[depth, c], z - 1))

    def arrive(step):
        for c in range(chunks):
            for g in range(step, min(2 * step, depth - 1) + 1):
                source = group_z(g)
                due = jnp.abs(source - z) == step

                @pl.when(due)
                def _():
                    remote(
                        token_region(source, c),
                        token_region(source, c),
                        a_send.at[g, c],
                        a_recv.at[source, c],
                        (me, partner),
                    ).wait_recv()

                target = jnp.where(source < z, z + 1, z - 1)
                ahead = due & (target >= 0) & (target < depth)
                copy = remote(
                    token_region(source, c),
                    token_region(source, c),
                    a_send.at[g, c],
                    a_recv.at[source, c],
                    (target * across + x, t),
                )

                @pl.when(ahead)
                def _():
                    copy.start()

                guarded.append((ahead, copy))

    slot_rows = lax.broadcasted_iota(jnp.int32, (cap, row_count), 0).astype(jnp.float32)

    def select(g):
        source = group_z(g)
        if g > 0:
            remote(
                key_rows.at[source], key_rows.at[source], k_send.at[g], k_recv.at[source], (me, partner)
            ).wait_recv()
        for d in list(range(1, across)) + [0]:
            there = z * across + lax.rem(x + d, across)
            chosen = jnp.where(
                slot_rows == key_rows[source, pl.ds(there, 1), :], 1.0, 0.0
            ).astype(jnp.bfloat16)
            value = jnp.dot(
                chosen, tokens[source], preferred_element_type=jnp.float32
            ).astype(jnp.bfloat16)
            if d == 0:
                piece[g * across, :, column(t, cols)] = value
            else:
                slots_out[g, d - 1] = value
                copy = remote(
                    slots_out.at[g, d - 1],
                    piece.at[g * across + d, :, column(t, cols)],
                    x_send.at[g, d - 1],
                    x_recv.at[g, d - 1],
                    (there, t),
                )
                copy.start()
                sends.append(copy)

    def fan_region(f, index):
        return piece.at[f, :, column(index, cols)]

    def fan_out(g, d):
        f = g * across + d
        region = fan_region(f, t)
        if d > 0:
            remote(
                region, region, x_send.at[g, d - 1], x_recv.at[g, d - 1], (me, partner)
            ).wait_recv()
        for e in range(1, chips):
            copy = remote(
                region, region, y_send.at[e, f], y_recv.at[e, f], (me, chip_at(e))
            )
            copy.start()
            sends.append(copy)
        copy = remote(region, region, p_send.at[0, f], p_recv.at[0, f], (me, partner))
        copy.start()
        sends.append(copy)

    def relay(g):
        for f in range(g * across, (g + 1) * across):
            for d in range(1, chips):
                source = chip_at(-d)
                region = fan_region(f, source)
                remote(
                    region, region, y_send.at[d, f], y_recv.at[d, f], (me, partner)
                ).wait_recv()
                copy = remote(region, region, p_send.at[d, f], p_recv.at[d, f], (me, partner))
                copy.start()
                sends.append(copy)

    def hid_region(g, index):
        return hid.at[g, :, column(index, ffn_local)]

    def up_stage(g):
        for f in range(g * across, (g + 1) * across):
            for d in range(chips):
                region = fan_region(f, chip_at(-d) + partner - t)
                remote(
                    region, region, p_send.at[d, f], p_recv.at[d, f], (me, partner)
                ).wait_recv()
        if g == 0:
            weight_copies[0].wait()
            weight_copies[1].wait()
        step = min(256, ffn_local)

        def tile(j, carry):
            rows = piece[pl.ds(g * across, across)].reshape(group_rows, tp * cols)
            at = pl.ds(pl.multiple_of(j * step, 128), step)
            gate_val = jnp.dot(rows, gate_w[:, at], preferred_element_type=jnp.float32)
            up_val = jnp.dot(rows, up_w[:, at], preferred_element_type=jnp.float32)
            hidden = (jax.nn.silu(gate_val) * up_val).astype(jnp.bfloat16)
            hid[g, :, pl.ds(pl.multiple_of(t * ffn_local + j * step, 128), step)] = hidden
            return carry

        lax.fori_loop(0, ffn_local // step, tile, 0)

    def send_hidden(g):
        region = hid_region(g, t)
        for d in range(1, chips):
            copy = remote(
                region, region, hy_send.at[d, g], hy_recv.at[d, g], (me, chip_at(d))
            )
            copy.start()
            sends.append(copy)
        copy = remote(region, region, hp_send.at[0, g], hp_recv.at[0, g], (me, partner))
        copy.start()
        sends.append(copy)

    def relay_hidden(g):
        for d in range(1, chips):
            region = hid_region(g, chip_at(-d))
            remote(
                region, region, hy_send.at[d, g], hy_recv.at[d, g], (me, partner)
            ).wait_recv()
            copy = remote(region, region, hp_send.at[d, g], hp_recv.at[d, g], (me, partner))
            copy.start()
            sends.append(copy)

    def down_stage(g, first=False):
        for d in range(chips):
            region = hid_region(g, chip_at(-d) + partner - t)
            remote(
                region, region, hp_send.at[d, g], hp_recv.at[d, g], (me, partner)
            ).wait_recv()
        if first:
            weight_copies[2].wait()
        step = min(256, cols)

        def tile(j, carry):
            at = pl.ds(pl.multiple_of(j * step, 128), step)
            value = jnp.dot(hid[g], down_w[:, at], preferred_element_type=jnp.float32)
            eo[pl.ds(g * across, across), :, at] = value.astype(jnp.bfloat16).reshape(
                across, cap, step
            )
            return carry

        lax.fori_loop(0, cols // step, tile, 0)
        for d in range(across):
            if g == 0 and d == 0:
                continue
            k = g * across + d
            copy = remote(
                eo.at[k],
                ret_ref.at[me],
                r_send.at[k],
                r_recv.at[me],
                (group_z(g) * across + lax.rem(x + across - d, across), t),
            )
            copy.start()
            sends.append(copy)

    last = depth - 1
    select(0)
    for d in range(across):
        fan_out(0, d)
    for s in range(1, depth):
        arrive(s)
        select(s)
        fan_out(s, 0)
        relay(s - 1)
        up_stage(s - 1)
        if s > 1:
            send_hidden(s - 1)
        for d in range(1, across):
            fan_out(s, d)
        if s > 2:
            relay_hidden(s - 2)
            down_stage(s - 2, s == 3)
    relay(last)
    up_stage(last)
    if last > 0:
        send_hidden(last)
    send_hidden(0)
    if last > 1:
        relay_hidden(last - 1)
        down_stage(last - 1, last == 2)
    if last > 0:
        relay_hidden(last)
        down_stage(last, last == 1)
    relay_hidden(0)
    down_stage(0, last == 0)

    slot_lanes = lax.broadcasted_iota(jnp.int32, (row_count, cap), 1).astype(jnp.float32)
    for g in range(depth):
        chosen = []
        for d in range(across):
            there = group_z(g) * across + lax.rem(x + d, across)
            own = g == 0 and d == 0
            if not own:
                k = g * across + d
                remote(
                    eo.at[k], ret_ref.at[there], r_send.at[k], r_recv.at[there], (me, partner)
                ).wait_recv()
            here = lanes == there
            key = jnp.sum(jnp.where(here, key_col[...], 0.0), axis=1, keepdims=True)
            weight = jnp.sum(jnp.where(here, mix_col[...], 0.0), axis=1, keepdims=True)
            slot_of = jnp.where(slot_lanes == key, 1.0, 0.0).astype(jnp.bfloat16)
            chosen.append((eo.at[0] if own else ret_ref.at[there], slot_of, weight))
        step = min(256, cols)

        def combine(j, carry):
            at = pl.ds(pl.multiple_of(j * step, 128), step)
            value = jnp.zeros((row_count, step), jnp.float32) if g == 0 else acc[:, at]
            for source, slot_of, weight in chosen:
                value = value + weight * jnp.dot(
                    slot_of, source[:, at], preferred_element_type=jnp.float32
                )
            if g == depth - 1:
                result_ref[:, at] = (resid[:, at].astype(jnp.float32) + value).astype(jnp.bfloat16)
            else:
                acc[:, at] = value
            return carry

        lax.fori_loop(0, cols // step, combine, 0)
    for copy in sends:
        copy.wait_send()
    for started, copy in guarded:
        pl.when(started)(copy.wait_send)


def whole_layer(blocks, weights):
    n, tp = lax.axis_size("sp"), lax.axis_size("tp")
    row_count, wide = blocks[0].shape
    cols = blocks[5].shape[1]
    cap = 4 * row_count // n
    chips = tp // 2
    rows = n * cap
    across = max(d for d in range(1, n + 1) if n % d == 0 and d * d <= n)
    depth = n // across
    chunks = 2
    projection, gate_weight, _, down_weight = weights
    width, ffn_local = gate_weight.shape[1], gate_weight.shape[2]
    ffn = down_weight.shape[1]
    dma = pltpu.SemaphoreType.DMA
    bf16, f32 = jnp.bfloat16, jnp.float32
    flops = 2 * rows * width * ffn_local * 2 + 2 * rows * ffn * cols
    return pl.pallas_call(
        functools.partial(expert_kernel, n, tp, across),
        out_shape=jax.ShapeDtypeStruct((row_count, cols), bf16),
        in_specs=[pl.BlockSpec(memory_space=pltpu.VMEM)] * len(blocks)
        + [pl.BlockSpec(memory_space=pl.ANY)] * len(weights),
        out_specs=pl.BlockSpec(memory_space=pltpu.VMEM),
        scratch_shapes=[
            pltpu.VMEM((depth, row_count, cols), bf16),
            pltpu.VMEM((depth, max(1, across - 1), cap, cols), bf16),
            pltpu.VMEM((n, cap, cols), bf16),
            pltpu.VMEM((row_count, wide * tp), bf16),
            pltpu.VMEM(projection.shape, bf16),
            pltpu.VMEM((row_count, cols), f32),
            pltpu.VMEM((row_count, cols), bf16),
            pltpu.VMEM((tp, 8, row_count), f32),
            pltpu.VMEM((row_count, 128), f32),
            pltpu.VMEM((depth, -(-n // 8) * 8, row_count), f32),
            pltpu.VMEM((row_count, 128), f32),
            pltpu.VMEM((16, wide), bf16),
            pltpu.VMEM((16, wide), bf16),
            pltpu.VMEM((8, 128), f32),
            pltpu.VMEM((n, cap, width), bf16),
            pltpu.VMEM((depth, rows // depth, ffn), bf16),
            pltpu.VMEM((n, cap, cols), bf16),
            pltpu.VMEM((width, ffn_local), bf16),
            pltpu.VMEM((width, ffn_local), bf16),
            pltpu.VMEM((ffn, cols), bf16),
            dma((4,)),
            dma((depth,)),
            dma((depth,)),
            dma((depth + 1, chunks)),
            dma((depth, chunks)),
            dma((depth, across)),
            dma((depth, across)),
            dma((chips, n)),
            dma((chips, n)),
            dma((chips, n)),
            dma((chips, n)),
            dma((chips, depth)),
            dma((chips, depth)),
            dma((chips, depth)),
            dma((chips, depth)),
            dma((n,)),
            dma((n,)),
            dma((3,)),
            dma((3,)),
            dma((chips,)),
            dma((chips,)),
            dma((chips,)),
            dma((chips,)),
            dma((tp,)),
            dma((tp,)),
        ],
        compiler_params=pltpu.CompilerParams(
            collective_id=0, has_side_effects=True, vmem_limit_bytes=56 * 1024 * 1024
        ),
        cost_estimate=pl.CostEstimate(
            flops=flops, bytes_accessed=3 * width * ffn_local * 2, transcendentals=0
        ),
        name="layer",
    )(*blocks, *weights)


def per_device(
    outer_gate,
    inner_gate,
    conv_input,
    conv_weight,
    doc_ids,
    output_weight,
    residual,
    norm_gain,
    expert_ids,
    group_weight,
    expert_weight,
    gate_weight,
    up_weight,
    down_weight,
):
    row_count = conv_input.shape[0]
    docs = jnp.broadcast_to(doc_ids.astype(jnp.float32)[:, None], (row_count, 128))
    mix_weight = (
        group_weight[:, None] * expert_weight / jnp.sum(expert_weight, axis=1, keepdims=True)
    )
    return whole_layer(
        (
            outer_gate,
            inner_gate,
            conv_input,
            conv_weight,
            docs,
            residual,
            norm_gain[None, :],
            expert_ids,
            mix_weight,
        ),
        (output_weight, gate_weight, up_weight, down_weight),
    )


def solution(mesh):
    return jax.shard_map(
        per_device,
        mesh=mesh,
        in_specs=(
            P("sp", "tp"),
            P("sp", "tp"),
            P("sp", "tp"),
            P(None, "tp"),
            P("sp"),
            P(None, "tp"),
            P("sp", "tp"),
            P("tp"),
            P("sp", None),
            P("sp"),
            P("sp", None),
            P("sp", None, "tp"),
            P("sp", None, "tp"),
            P("sp", None, "tp"),
        ),
        out_specs=P("sp", "tp"),
        check_vma=False,
    )
```

```python
import functools

import jax
import jax.numpy as jnp
from jax import lax
from jax.experimental import pallas as pl
from jax.experimental.pallas import tpu as pltpu
from jax.sharding import PartitionSpec as P

EPS = 1e-06
MESH = pl.DeviceIdType.MESH


def remote(src, dst, send_sem, recv_sem, device):
    return pltpu.make_async_remote_copy(
        src_ref=src,
        dst_ref=dst,
        send_sem=send_sem,
        recv_sem=recv_sem,
        device_id=device,
        device_id_type=MESH,
    )


def expert_kernel(
    n,
    tp,
    across,
    outer_ref,
    inner_ref,
    conv_ref,
    taps_ref,
    docs_ref,
    residual_ref,
    gain_ref,
    ids_ref,
    group_ref,
    mix_ref,
    proj_hbm,
    gate_hbm,
    up_hbm,
    down_hbm,
    result_ref,
    tokens,
    slots_out,
    ret_ref,
    branch,
    proj_w,
    acc,
    resid,
    squares,
    total,
    scales,
    gain_row,
    key_col,
    key_rows,
    mix_col,
    docs_rows,
    halo_inner,
    halo_conv,
    halo_docs,
    piece,
    hid,
    eo,
    gate_w,
    up_w,
    down_w,
    w_sem,
    k_send,
    k_recv,
    c_send,
    c_recv,
    a_send,
    a_recv,
    x_send,
    x_recv,
    y_send,
    y_recv,
    p_send,
    p_recv,
    hy_send,
    hy_recv,
    hp_send,
    hp_recv,
    r_send,
    r_recv,
    h_send,
    h_recv,
    by_send,
    by_recv,
    bp_send,
    bp_recv,
    s_send,
    s_recv,
):
    me = lax.axis_index("sp")
    t = lax.axis_index("tp")
    chips = tp // 2
    y, core = lax.div(t, 2), lax.rem(t, 2)
    partner = t + 1 - 2 * core
    cap, cols = ret_ref.shape[1], ret_ref.shape[2]
    ffn_local = gate_w.shape[1]
    depth, group_rows = hid.shape[0], hid.shape[1]
    z, x = lax.div(me, across), lax.rem(me, across)
    chunks = a_recv.shape[1]
    key_count = key_rows.shape[1]

    near = jnp.minimum(z, depth - 1 - z)
    low = 2 * z < depth

    def group_z(g):
        if g == 0:
            return z
        step = (g + 1) // 2
        outward = step if g % 2 else -step
        close = jnp.where(low, z + outward, z - outward)
        far = jnp.where(low, g, depth - 1 - g)
        return jnp.where(g <= 2 * near, close, far)

    def column(index, width):
        return pl.ds(pl.multiple_of(index * width, 128), width)

    def chip_at(delta):
        return lax.rem(y + delta + chips, chips) * 2 + core

    weight_copies = [
        pltpu.make_async_copy(source, target, w_sem.at[i])
        for i, (source, target) in enumerate(
            (
                (gate_hbm.at[0], gate_w),
                (up_hbm.at[0], up_w),
                (down_hbm.at[0], down_w),
                (proj_hbm, proj_w),
            )
        )
    ]
    for i in (3, 0, 1, 2):
        weight_copies[i].start()

    barrier = pltpu.get_barrier_semaphore()
    for k in range(1, n):
        pl.semaphore_signal(
            barrier, inc=1, device_id=(lax.rem(me + k, n), t), device_id_type=MESH
        )
    for d in range(1, tp):
        pl.semaphore_signal(
            barrier, inc=1, device_id=(me, lax.rem(t + d, tp)), device_id_type=MESH
        )

    sends = []
    row_count = residual_ref.shape[0]
    wide = branch.shape[1] // tp
    half = row_count // 2

    experts = lax.broadcasted_iota(jnp.int32, (128, row_count), 0)
    is_first, is_second = experts == ids_ref[0:1, :], experts == ids_ref[1:2, :]
    pair = mix_ref[...]
    mix = group_ref[...].reshape(1, row_count) * pair / (pair[0:1] + pair[1:2])
    mix_rows = jnp.where(is_first, mix[0:1], 0.0) + jnp.where(is_second, mix[1:2], 0.0)
    mix_col[...] = mix_rows.T
    member = jnp.where(is_first, 1.0, 0.0) + jnp.where(is_second, 1.0, 0.0)
    earlier = jnp.where(
        lax.broadcasted_iota(jnp.int32, (row_count, row_count), 0)
        < lax.broadcasted_iota(jnp.int32, (row_count, row_count), 1),
        1.0,
        0.0,
    ).astype(jnp.bfloat16)
    ranks = jnp.dot(member.astype(jnp.bfloat16), earlier, preferred_element_type=jnp.float32)
    keys = jnp.where(member > 0.5, ranks, -1.0)
    key_col[...] = keys.T
    key_rows[me] = keys[0:key_count]
    gain_row[...] = gain_ref[...].reshape(1, cols).astype(jnp.float32)

    docs = jnp.broadcast_to(docs_ref[...].reshape(1, row_count).astype(jnp.float32), (8, row_count))
    docs_rows[...] = docs
    position = lax.broadcasted_iota(jnp.int32, (8, row_count), 1)

    def as_column(mask):
        rows = jnp.where(mask, 1.0, 0.0)[0:1]
        return jnp.broadcast_to(rows, (128, rows.shape[1])).T > 0.5

    same_one = as_column((pltpu.roll(docs, 1, 1) == docs) & (position >= 1))
    same_two = as_column((pltpu.roll(docs, 2, 1) == docs) & (position >= 2))

    def weigh(at, products, one, two, first, second, outer):
        taps = taps_ref[:, at].astype(jnp.float32)
        conv = taps[2:3] * products
        conv = conv + jnp.where(first, taps[1:2] * one, 0.0)
        conv = conv + jnp.where(second, taps[0:1] * two, 0.0)
        return (outer.astype(jnp.float32) * conv).astype(jnp.bfloat16)

    def conv_tile(j, carry):
        at = pl.ds(pl.multiple_of(j * 128, 128), 128)
        products = inner_ref[:, at].astype(jnp.float32) * conv_ref[:, at].astype(jnp.float32)
        one, two = pltpu.roll(products, 1, 0), pltpu.roll(products, 2, 0)
        value = weigh(at, products, one, two, same_one, same_two, outer_ref[:, at])
        branch[:, pl.ds(pl.multiple_of(t * wide + j * 128, 128), 128)] = value
        return carry

    lax.fori_loop(0, wide // 128, conv_tile, 0)

    pl.semaphore_wait(barrier, n - 1 + tp - 1)

    halos = []
    following = (lax.rem(me + 1, n), t)
    for i, (source, target) in enumerate(
        (
            (inner_ref.at[pl.ds(row_count - 16, 16)], halo_inner),
            (conv_ref.at[pl.ds(row_count - 16, 16)], halo_conv),
            (docs_rows.at[:, pl.ds(row_count - 128, 128)], halo_docs),
        )
    ):
        copy = remote(source, target, h_send.at[i], h_recv.at[i], following)
        copy.start()
        halos.append(copy)
        sends.append(copy)

    def branch_region(index, h):
        return branch.at[pl.ds(h * half, half), column(index, wide)]

    def send_branch(h):
        region = branch_region(t, h)
        for d in range(1, chips):
            copy = remote(region, region, by_send.at[d, h], by_recv.at[d, h], (me, chip_at(d)))
            copy.start()
            sends.append(copy)
        copy = remote(region, region, bp_send.at[0, h], bp_recv.at[0, h], (me, partner))
        copy.start()
        sends.append(copy)

    send_branch(1)
    for d in range(1, n):
        copy = remote(
            key_rows.at[me],
            key_rows.at[me],
            k_send.at[d],
            k_recv.at[me],
            (lax.rem(me + d, n), t),
        )
        copy.start()
        sends.append(copy)

    for copy in halos:
        copy.wait_recv()
    lane = lax.broadcasted_iota(jnp.int32, (8, 128), 1)
    near_docs = docs_rows[:, 0:128]
    past_docs = jnp.where(me > 0, halo_docs[...], -1.0)
    docs_one = jnp.where(lane < 1, pltpu.roll(past_docs, 1, 1), pltpu.roll(near_docs, 1, 1))
    docs_two = jnp.where(lane < 2, pltpu.roll(past_docs, 2, 1), pltpu.roll(near_docs, 2, 1))
    edge_one = as_column(docs_one == near_docs)[0:16]
    edge_two = as_column(docs_two == near_docs)[0:16]
    row_at = lax.broadcasted_iota(jnp.int32, (16, 1), 0)
    for j in range(wide // 128):
        at = pl.ds(j * 128, 128)
        products = inner_ref[0:16, at].astype(jnp.float32) * conv_ref[0:16, at].astype(jnp.float32)
        before = halo_inner[:, at].astype(jnp.float32) * halo_conv[:, at].astype(jnp.float32)
        one = jnp.where(row_at < 1, pltpu.roll(before, 1, 0), pltpu.roll(products, 1, 0))
        two = jnp.where(row_at < 2, pltpu.roll(before, 2, 0), pltpu.roll(products, 2, 0))
        value = weigh(at, products, one, two, edge_one, edge_two, outer_ref[0:16, at])
        branch[0:16, pl.ds(pl.multiple_of(t * wide + j * 128, 128), 128)] = value
    send_branch(0)
    weight_copies[3].wait()

    chunk = cols // chunks
    step_cols = min(256, chunk)

    def project(index, first=False, c=None):
        def tile(j, carry):
            at = pl.ds(pl.multiple_of(j * step_cols, 128), step_cols)
            rows = pl.ds(pl.multiple_of(index * wide, 128), wide)
            value = jnp.dot(
                branch[:, column(index, wide)], proj_w[rows, at], preferred_element_type=jnp.float32
            )
            acc[:, at] = value if first else acc[:, at] + value
            return carry

        tiles = chunk // step_cols
        lo, hi = (0, chunks * tiles) if c is None else (c * tiles, (c + 1) * tiles)
        lax.fori_loop(lo, hi, tile, 0)

    def branch_arrived(index, sem, h):
        region = branch_region(index, h)
        return remote(region, region, sem, sem, (me, partner))

    project(t, True)
    for h in (1, 0):
        branch_arrived(partner, bp_recv.at[0, h], h).wait_recv()
    project(partner)
    for d in range(1, chips):
        source = chip_at(-d)
        for h in (1, 0):
            branch_arrived(source, by_recv.at[d, h], h).wait_recv()
            region = branch_region(source, h)
            copy = remote(region, region, bp_send.at[d, h], bp_recv.at[d, h], (me, partner))
            copy.start()
            sends.append(copy)
        project(source)
    for d in range(1, chips):
        source = chip_at(-d) + partner - t
        for h in (1, 0):
            branch_arrived(source, bp_recv.at[d, h], h).wait_recv()
        if d < chips - 1:
            project(source)

    guarded = []

    def token_region(index, c):
        return tokens.at[index, :, pl.ds(c * chunk, chunk)]

    def pass_on(index, c, sem, target):
        inside = (target >= 0) & (target < depth)
        copy = remote(
            token_region(index, c),
            token_region(index, c),
            sem,
            a_recv.at[index, c],
            (target * across + x, t),
        )

        @pl.when(inside)
        def _():
            copy.start()

        return inside, copy

    total[...] = jnp.zeros_like(total)

    def resid_tile(j, carry):
        at = pl.ds(pl.multiple_of(j * 128, 128), 128)
        value = (residual_ref[:, at].astype(jnp.float32) + acc[:, at]).astype(jnp.bfloat16)
        resid[:, at] = value
        value = value.astype(jnp.float32)
        total[...] += value * value
        tokens[z, :, at] = (value * gain_row[:, at]).astype(jnp.bfloat16)
        return carry

    for c in range(chunks):
        if chips > 1:
            project(source, c=c)
        lax.fori_loop(c * chunk // 128, (c + 1) * chunk // 128, resid_tile, 0)
        guarded.append(pass_on(z, c, a_send.at[0, c], z + 1))
        guarded.append(pass_on(z, c, a_send.at[depth, c], z - 1))
    squares[t] = jnp.broadcast_to(
        jnp.sum(total[...].T, axis=0, keepdims=True), (8, row_count)
    )
    for d in range(1, tp):
        copy = remote(
            squares.at[t], squares.at[t], s_send.at[d], s_recv.at[d], (me, lax.rem(t + d, tp))
        )
        copy.start()
        sends.append(copy)

    def share_scale():
        for d in range(1, tp):
            other = lax.rem(t + tp - d, tp)
            remote(
                squares.at[other], squares.at[other], s_send.at[d], s_recv.at[d], (me, other)
            ).wait_recv()
        total_sq = jnp.sum(squares[...], axis=0)
        scales[me] = lax.rsqrt(total_sq / (tp * cols) + EPS)
        for d in range(1, n):
            copy = remote(
                scales.at[me],
                scales.at[me],
                c_send.at[d],
                c_recv.at[me],
                (lax.rem(me + d, n), t),
            )
            copy.start()
            sends.append(copy)

    def arrive(step):
        for c in range(chunks):
            for g in range(step, min(2 * step, depth - 1) + 1):
                source = group_z(g)
                due = jnp.abs(source - z) == step

                @pl.when(due)
                def _():
                    remote(
                        token_region(source, c),
                        token_region(source, c),
                        a_send.at[g, c],
                        a_recv.at[source, c],
                        (me, partner),
                    ).wait_recv()

                target = jnp.where(source < z, z + 1, z - 1)
                ahead = due & (target >= 0) & (target < depth)
                copy = remote(
                    token_region(source, c),
                    token_region(source, c),
                    a_send.at[g, c],
                    a_recv.at[source, c],
                    (target * across + x, t),
                )

                @pl.when(ahead)
                def _():
                    copy.start()

                guarded.append((ahead, copy))

    slot_rows = lax.broadcasted_iota(jnp.int32, (cap, row_count), 0).astype(jnp.float32)

    def wait_keys(origin):
        remote(
            key_rows.at[origin], key_rows.at[origin], k_send.at[1], k_recv.at[origin], (me, partner)
        ).wait_recv()

    def slot_scale(g, d):
        origin = group_z(g) * across + lax.rem(x + across - d, across)
        if d > 0:
            wait_keys(origin)
        if g > 0 or d > 0:
            remote(
                scales.at[origin], scales.at[origin], c_send.at[1], c_recv.at[origin], (me, partner)
            ).wait_recv()
        mine = slot_rows == key_rows[origin, pl.ds(me, 1), :]
        return jnp.sum(jnp.where(mine, scales[origin, 0:1, :], 0.0), axis=1, keepdims=True)

    def select(g):
        source = group_z(g)
        origin = source * across + x
        if g > 0:
            wait_keys(origin)
        for d in list(range(1, across)) + [0]:
            there = z * across + lax.rem(x + d, across)
            chosen = jnp.where(
                slot_rows == key_rows[origin, pl.ds(there, 1), :], 1.0, 0.0
            ).astype(jnp.bfloat16)
            value = jnp.dot(
                chosen, tokens[source], preferred_element_type=jnp.float32
            ).astype(jnp.bfloat16)
            if d == 0:
                piece[g * across, :, column(t, cols)] = value
            else:
                slots_out[g, d - 1] = value
                copy = remote(
                    slots_out.at[g, d - 1],
                    piece.at[g * across + d, :, column(t, cols)],
                    x_send.at[g, d - 1],
                    x_recv.at[g, d - 1],
                    (there, t),
                )
                copy.start()
                sends.append(copy)

    def fan_region(f, index):
        return piece.at[f, :, column(index, cols)]

    def fan_out(g, d):
        f = g * across + d
        region = fan_region(f, t)
        if d > 0:
            remote(
                region, region, x_send.at[g, d - 1], x_recv.at[g, d - 1], (me, partner)
            ).wait_recv()
        for e in range(1, chips):
            copy = remote(
                region, region, y_send.at[e, f], y_recv.at[e, f], (me, chip_at(e))
            )
            copy.start()
            sends.append(copy)
        copy = remote(region, region, p_send.at[0, f], p_recv.at[0, f], (me, partner))
        copy.start()
        sends.append(copy)

    def relay(g):
        for f in range(g * across, (g + 1) * across):
            for d in range(1, chips):
                source = chip_at(-d)
                region = fan_region(f, source)
                remote(
                    region, region, y_send.at[d, f], y_recv.at[d, f], (me, partner)
                ).wait_recv()
                copy = remote(region, region, p_send.at[d, f], p_recv.at[d, f], (me, partner))
                copy.start()
                sends.append(copy)

    def hid_region(g, index):
        return hid.at[g, :, column(index, ffn_local)]

    def up_stage(g):
        for f in range(g * across, (g + 1) * across):
            for d in range(chips):
                region = fan_region(f, chip_at(-d) + partner - t)
                remote(
                    region, region, p_send.at[d, f], p_recv.at[d, f], (me, partner)
                ).wait_recv()
        if g == 0:
            weight_copies[0].wait()
            weight_copies[1].wait()
        scale = jnp.concatenate([slot_scale(g, d) for d in range(across)], axis=0)
        step = min(256, ffn_local)

        def tile(j, carry):
            rows = piece[pl.ds(g * across, across)].reshape(group_rows, tp * cols)
            at = pl.ds(pl.multiple_of(j * step, 128), step)
            gate_val = jnp.dot(rows, gate_w[:, at], preferred_element_type=jnp.float32)
            up_val = jnp.dot(rows, up_w[:, at], preferred_element_type=jnp.float32)
            hidden = (jax.nn.silu(gate_val * scale) * (up_val * scale)).astype(jnp.bfloat16)
            hid[g, :, pl.ds(pl.multiple_of(t * ffn_local + j * step, 128), step)] = hidden
            return carry

        lax.fori_loop(0, ffn_local // step, tile, 0)

    def send_hidden(g):
        region = hid_region(g, t)
        for d in range(1, chips):
            copy = remote(
                region, region, hy_send.at[d, g], hy_recv.at[d, g], (me, chip_at(d))
            )
            copy.start()
            sends.append(copy)
        copy = remote(region, region, hp_send.at[0, g], hp_recv.at[0, g], (me, partner))
        copy.start()
        sends.append(copy)

    def relay_hidden(g):
        for d in range(1, chips):
            region = hid_region(g, chip_at(-d))
            remote(
                region, region, hy_send.at[d, g], hy_recv.at[d, g], (me, partner)
            ).wait_recv()
            copy = remote(region, region, hp_send.at[d, g], hp_recv.at[d, g], (me, partner))
            copy.start()
            sends.append(copy)

    def down_stage(g, first=False):
        for d in range(chips):
            region = hid_region(g, chip_at(-d) + partner - t)
            remote(
                region, region, hp_send.at[d, g], hp_recv.at[d, g], (me, partner)
            ).wait_recv()
        if first:
            weight_copies[2].wait()
        step = min(256, cols)

        def tile(j, carry):
            at = pl.ds(pl.multiple_of(j * step, 128), step)
            value = jnp.dot(hid[g], down_w[:, at], preferred_element_type=jnp.float32)
            eo[pl.ds(g * across, across), :, at] = value.astype(jnp.bfloat16).reshape(
                across, cap, step
            )
            return carry

        lax.fori_loop(0, cols // step, tile, 0)
        for d in range(across):
            if g == 0 and d == 0:
                continue
            k = g * across + d
            copy = remote(
                eo.at[k],
                ret_ref.at[me],
                r_send.at[k],
                r_recv.at[me],
                (group_z(g) * across + lax.rem(x + across - d, across), t),
            )
            copy.start()
            sends.append(copy)

    last = depth - 1
    select(0)
    fan_out(0, 0)
    share_scale()
    for d in range(1, across):
        fan_out(0, d)
    for s in range(1, depth):
        arrive(s)
        select(s)
        fan_out(s, 0)
        relay(s - 1)
        up_stage(s - 1)
        if s > 1:
            send_hidden(s - 1)
        for d in range(1, across):
            fan_out(s, d)
        if s > 2:
            relay_hidden(s - 2)
            down_stage(s - 2, s == 3)
    relay(last)
    up_stage(last)
    if last > 0:
        send_hidden(last)
    send_hidden(0)
    if last > 1:
        relay_hidden(last - 1)
        down_stage(last - 1, last == 2)
    if last > 0:
        relay_hidden(last)
        down_stage(last, last == 1)
    relay_hidden(0)
    down_stage(0, last == 0)

    lanes = lax.broadcasted_iota(jnp.int32, (row_count, 128), 1)
    slot_lanes = lax.broadcasted_iota(jnp.int32, (row_count, cap), 1).astype(jnp.float32)
    for g in range(depth):
        chosen = []
        for d in range(across):
            there = group_z(g) * across + lax.rem(x + d, across)
            own = g == 0 and d == 0
            if not own:
                k = g * across + d
                remote(
                    eo.at[k], ret_ref.at[there], r_send.at[k], r_recv.at[there], (me, partner)
                ).wait_recv()
            here = lanes == there
            key = jnp.sum(jnp.where(here, key_col[...], 0.0), axis=1, keepdims=True)
            weight = jnp.sum(jnp.where(here, mix_col[...], 0.0), axis=1, keepdims=True)
            slot_of = jnp.where(slot_lanes == key, 1.0, 0.0).astype(jnp.bfloat16)
            chosen.append((eo.at[0] if own else ret_ref.at[there], slot_of, weight))
        step = min(256, cols)

        def combine(j, carry):
            at = pl.ds(pl.multiple_of(j * step, 128), step)
            value = jnp.zeros((row_count, step), jnp.float32) if g == 0 else acc[:, at]
            for source, slot_of, weight in chosen:
                value = value + weight * jnp.dot(
                    slot_of, source[:, at], preferred_element_type=jnp.float32
                )
            if g == depth - 1:
                result_ref[:, at] = (resid[:, at].astype(jnp.float32) + value).astype(jnp.bfloat16)
            else:
                acc[:, at] = value
            return carry

        lax.fori_loop(0, cols // step, combine, 0)
    for copy in sends:
        copy.wait_send()
    for started, copy in guarded:
        pl.when(started)(copy.wait_send)


def whole_layer(blocks, weights):
    n, tp = lax.axis_size("sp"), lax.axis_size("tp")
    row_count, wide = blocks[0].shape
    cols = blocks[5].shape[1]
    cap = 4 * row_count // n
    chips = tp // 2
    rows = n * cap
    across = max(d for d in range(1, n + 1) if n % d == 0 and d * d <= n)
    depth = n // across
    chunks = 2
    projection, gate_weight, _, down_weight = weights
    width, ffn_local = gate_weight.shape[1], gate_weight.shape[2]
    ffn = down_weight.shape[1]
    dma = pltpu.SemaphoreType.DMA
    bf16, f32 = jnp.bfloat16, jnp.float32
    flops = 2 * rows * width * ffn_local * 2 + 2 * rows * ffn * cols
    return pl.pallas_call(
        functools.partial(expert_kernel, n, tp, across),
        out_shape=jax.ShapeDtypeStruct((row_count, cols), bf16),
        in_specs=[pl.BlockSpec(memory_space=pltpu.VMEM)] * len(blocks)
        + [pl.BlockSpec(memory_space=pl.ANY)] * len(weights),
        out_specs=pl.BlockSpec(memory_space=pltpu.VMEM),
        scratch_shapes=[
            pltpu.VMEM((depth, row_count, cols), bf16),
            pltpu.VMEM((depth, max(1, across - 1), cap, cols), bf16),
            pltpu.VMEM((n, cap, cols), bf16),
            pltpu.VMEM((row_count, wide * tp), bf16),
            pltpu.VMEM(projection.shape, bf16),
            pltpu.VMEM((row_count, cols), f32),
            pltpu.VMEM((row_count, cols), bf16),
            pltpu.VMEM((tp, 8, row_count), f32),
            pltpu.VMEM((row_count, 128), f32),
            pltpu.VMEM((n, 8, row_count), f32),
            pltpu.VMEM((1, cols), f32),
            pltpu.VMEM((row_count, 128), f32),
            pltpu.VMEM((n, -(-n // 8) * 8, row_count), f32),
            pltpu.VMEM((row_count, 128), f32),
            pltpu.VMEM((8, row_count), f32),
            pltpu.VMEM((16, wide), bf16),
            pltpu.VMEM((16, wide), bf16),
            pltpu.VMEM((8, 128), f32),
            pltpu.VMEM((n, cap, width), bf16),
            pltpu.VMEM((depth, rows // depth, ffn), bf16),
            pltpu.VMEM((n, cap, cols), bf16),
            pltpu.VMEM((width, ffn_local), bf16),
            pltpu.VMEM((width, ffn_local), bf16),
            pltpu.VMEM((ffn, cols), bf16),
            dma((4,)),
            dma((n,)),
            dma((n,)),
            dma((n,)),
            dma((n,)),
            dma((depth + 1, chunks)),
            dma((depth, chunks)),
            dma((depth, across)),
            dma((depth, across)),
            dma((chips, n)),
            dma((chips, n)),
            dma((chips, n)),
            dma((chips, n)),
            dma((chips, depth)),
            dma((chips, depth)),
            dma((chips, depth)),
            dma((chips, depth)),
            dma((n,)),
            dma((n,)),
            dma((3,)),
            dma((3,)),
            dma((chips, 2)),
            dma((chips, 2)),
            dma((chips, 2)),
            dma((chips, 2)),
            dma((tp,)),
            dma((tp,)),
        ],
        compiler_params=pltpu.CompilerParams(
            collective_id=0, has_side_effects=True, vmem_limit_bytes=56 * 1024 * 1024
        ),
        cost_estimate=pl.CostEstimate(
            flops=flops, bytes_accessed=3 * width * ffn_local * 2, transcendentals=0
        ),
        name="layer",
    )(*blocks, *weights)


def per_device(
    outer_gate,
    inner_gate,
    conv_input,
    conv_weight,
    doc_ids,
    output_weight,
    residual,
    norm_gain,
    expert_ids,
    group_weight,
    expert_weight,
    gate_weight,
    up_weight,
    down_weight,
):
    return whole_layer(
        (
            outer_gate,
            inner_gate,
            conv_input,
            conv_weight,
            doc_ids,
            residual,
            norm_gain,
            expert_ids.T,
            group_weight,
            expert_weight.T,
        ),
        (output_weight, gate_weight, up_weight, down_weight),
    )


def solution(mesh):
    return jax.shard_map(
        per_device,
        mesh=mesh,
        in_specs=(
            P("sp", "tp"),
            P("sp", "tp"),
            P("sp", "tp"),
            P(None, "tp"),
            P("sp"),
            P(None, "tp"),
            P("sp", "tp"),
            P("tp"),
            P("sp", None),
            P("sp"),
            P("sp", None),
            P("sp", None, "tp"),
            P("sp", None, "tp"),
            P("sp", None, "tp"),
        ),
        out_specs=P("sp", "tp"),
        check_vma=False,
    )
```

```python
import functools

import jax
import jax.numpy as jnp
from jax import lax
from jax.experimental import pallas as pl
from jax.experimental.pallas import tpu as pltpu
from jax.sharding import PartitionSpec as P

EPS = 1e-06
MESH = pl.DeviceIdType.MESH


def remote(src, dst, send_sem, recv_sem, device):
    return pltpu.make_async_remote_copy(
        src_ref=src,
        dst_ref=dst,
        send_sem=send_sem,
        recv_sem=recv_sem,
        device_id=device,
        device_id_type=MESH,
    )


def expert_kernel(
    n,
    tp,
    across,
    outer_ref,
    inner_ref,
    conv_ref,
    taps_ref,
    docs_ref,
    residual_ref,
    gain_ref,
    ids_ref,
    group_ref,
    mix_ref,
    proj_hbm,
    gate_hbm,
    up_hbm,
    down_hbm,
    result_ref,
    tokens,
    early,
    slots_out,
    ret_ref,
    branch,
    proj_w,
    acc,
    resid,
    squares,
    total,
    scales,
    gain_row,
    key_col,
    key_rows,
    mix_col,
    docs_rows,
    halo_inner,
    halo_conv,
    halo_docs,
    piece,
    hid,
    eo,
    gate_w,
    up_w,
    down_w,
    w_sem,
    k_send,
    k_recv,
    c_send,
    c_recv,
    e_send,
    e_recv,
    a_send,
    a_recv,
    x_send,
    x_recv,
    y_send,
    y_recv,
    p_send,
    p_recv,
    hy_send,
    hy_recv,
    hp_send,
    hp_recv,
    r_send,
    r_recv,
    h_send,
    h_recv,
    by_send,
    by_recv,
    bp_send,
    bp_recv,
    s_send,
    s_recv,
):
    me = lax.axis_index("sp")
    t = lax.axis_index("tp")
    chips = tp // 2
    y, core = lax.div(t, 2), lax.rem(t, 2)
    partner = t + 1 - 2 * core
    cap, cols = ret_ref.shape[1], ret_ref.shape[2]
    ffn_local = gate_w.shape[1]
    depth, group_rows = hid.shape[0], hid.shape[1]
    z, x = lax.div(me, across), lax.rem(me, across)
    ahead_cols = early.shape[2] if e_send.shape[0] > 1 else 0
    chunks = x_recv.shape[2] - 1
    last = depth - 1
    pieces = chunks + (1 if ahead_cols else 0)
    key_count = key_rows.shape[1]

    near = jnp.minimum(z, depth - 1 - z)
    low = 2 * z < depth

    def group_z(g):
        if g == 0:
            return z
        step = (g + 1) // 2
        outward = step if g % 2 else -step
        close = jnp.where(low, z + outward, z - outward)
        return jnp.where(g <= 2 * near, close, jnp.where(low, g, depth - 1 - g))

    def is_early(g):
        return jnp.abs(group_z(g) - z) < g

    def column(index, width):
        return pl.ds(pl.multiple_of(index * width, 128), width)

    def chip_at(delta):
        return lax.rem(y + delta + chips, chips) * 2 + core

    weight_copies = [
        pltpu.make_async_copy(source, target, w_sem.at[i])
        for i, (source, target) in enumerate(
            (
                (gate_hbm.at[0], gate_w),
                (up_hbm.at[0], up_w),
                (down_hbm.at[0], down_w),
                (proj_hbm, proj_w),
            )
        )
    ]
    for i in (3, 0, 1, 2):
        weight_copies[i].start()

    barrier = pltpu.get_barrier_semaphore()
    for k in range(1, n):
        pl.semaphore_signal(
            barrier, inc=1, device_id=(lax.rem(me + k, n), t), device_id_type=MESH
        )
    for d in range(1, tp):
        pl.semaphore_signal(
            barrier, inc=1, device_id=(me, lax.rem(t + d, tp)), device_id_type=MESH
        )

    sends = []
    row_count = residual_ref.shape[0]
    wide = branch.shape[1] // tp
    half = row_count // 2

    experts = lax.broadcasted_iota(jnp.int32, (128, row_count), 0)
    is_first, is_second = experts == ids_ref[0:1, :], experts == ids_ref[1:2, :]
    pair = mix_ref[...]
    mix = group_ref[...].reshape(1, row_count) * pair / (pair[0:1] + pair[1:2])
    mix_rows = jnp.where(is_first, mix[0:1], 0.0) + jnp.where(is_second, mix[1:2], 0.0)
    mix_col[...] = mix_rows.T
    member = jnp.where(is_first, 1.0, 0.0) + jnp.where(is_second, 1.0, 0.0)
    earlier = jnp.where(
        lax.broadcasted_iota(jnp.int32, (row_count, row_count), 0)
        < lax.broadcasted_iota(jnp.int32, (row_count, row_count), 1),
        1.0,
        0.0,
    ).astype(jnp.bfloat16)
    ranks = jnp.dot(member.astype(jnp.bfloat16), earlier, preferred_element_type=jnp.float32)
    keys = jnp.where(member > 0.5, ranks, -1.0)
    key_col[...] = keys.T
    key_rows[me] = keys[0:key_count]
    gain_row[...] = gain_ref[...].reshape(1, cols).astype(jnp.float32)

    docs = jnp.broadcast_to(docs_ref[...].reshape(1, row_count).astype(jnp.float32), (8, row_count))
    docs_rows[...] = docs
    position = lax.broadcasted_iota(jnp.int32, (8, row_count), 1)

    def as_column(mask):
        rows = jnp.where(mask, 1.0, 0.0)[0:1]
        return jnp.broadcast_to(rows, (128, rows.shape[1])).T > 0.5

    same_one = as_column((pltpu.roll(docs, 1, 1) == docs) & (position >= 1))
    same_two = as_column((pltpu.roll(docs, 2, 1) == docs) & (position >= 2))

    def weigh(at, products, one, two, first, second, outer):
        taps = taps_ref[:, at].astype(jnp.float32)
        conv = taps[2:3] * products
        conv = conv + jnp.where(first, taps[1:2] * one, 0.0)
        conv = conv + jnp.where(second, taps[0:1] * two, 0.0)
        return (outer.astype(jnp.float32) * conv).astype(jnp.bfloat16)

    def conv_tile(j, carry):
        at = pl.ds(pl.multiple_of(j * 128, 128), 128)
        products = inner_ref[:, at].astype(jnp.float32) * conv_ref[:, at].astype(jnp.float32)
        one, two = pltpu.roll(products, 1, 0), pltpu.roll(products, 2, 0)
        value = weigh(at, products, one, two, same_one, same_two, outer_ref[:, at])
        branch[:, pl.ds(pl.multiple_of(t * wide + j * 128, 128), 128)] = value
        return carry

    lax.fori_loop(0, wide // 128, conv_tile, 0)

    pl.semaphore_wait(barrier, n - 1 + tp - 1)

    halos = []
    following = (lax.rem(me + 1, n), t)
    for i, (source, target) in enumerate(
        (
            (inner_ref.at[pl.ds(row_count - 16, 16)], halo_inner),
            (conv_ref.at[pl.ds(row_count - 16, 16)], halo_conv),
            (docs_rows.at[:, pl.ds(row_count - 128, 128)], halo_docs),
        )
    ):
        copy = remote(source, target, h_send.at[i], h_recv.at[i], following)
        copy.start()
        halos.append(copy)
        sends.append(copy)

    def branch_region(index, h):
        return branch.at[pl.ds(h * half, half), column(index, wide)]

    def send_branch(h):
        region = branch_region(t, h)
        for d in range(1, chips):
            copy = remote(region, region, by_send.at[d, h], by_recv.at[d, h], (me, chip_at(d)))
            copy.start()
            sends.append(copy)
        copy = remote(region, region, bp_send.at[0, h], bp_recv.at[0, h], (me, partner))
        copy.start()
        sends.append(copy)

    send_branch(1)
    for d in range(1, n):
        copy = remote(
            key_rows.at[me],
            key_rows.at[me],
            k_send.at[d],
            k_recv.at[me],
            (lax.rem(me + d, n), t),
        )
        copy.start()
        sends.append(copy)

    for copy in halos:
        copy.wait_recv()
    lane = lax.broadcasted_iota(jnp.int32, (8, 128), 1)
    near_docs = docs_rows[:, 0:128]
    past_docs = jnp.where(me > 0, halo_docs[...], -1.0)
    docs_one = jnp.where(lane < 1, pltpu.roll(past_docs, 1, 1), pltpu.roll(near_docs, 1, 1))
    docs_two = jnp.where(lane < 2, pltpu.roll(past_docs, 2, 1), pltpu.roll(near_docs, 2, 1))
    edge_one = as_column(docs_one == near_docs)[0:16]
    edge_two = as_column(docs_two == near_docs)[0:16]
    row_at = lax.broadcasted_iota(jnp.int32, (16, 1), 0)
    for j in range(wide // 128):
        at = pl.ds(j * 128, 128)
        products = inner_ref[0:16, at].astype(jnp.float32) * conv_ref[0:16, at].astype(jnp.float32)
        before = halo_inner[:, at].astype(jnp.float32) * halo_conv[:, at].astype(jnp.float32)
        one = jnp.where(row_at < 1, pltpu.roll(before, 1, 0), pltpu.roll(products, 1, 0))
        two = jnp.where(row_at < 2, pltpu.roll(before, 2, 0), pltpu.roll(products, 2, 0))
        value = weigh(at, products, one, two, edge_one, edge_two, outer_ref[0:16, at])
        branch[0:16, pl.ds(pl.multiple_of(t * wide + j * 128, 128), 128)] = value
    send_branch(0)
    weight_copies[3].wait()

    chunk = cols // chunks
    hid_step = ffn_local // hy_send.shape[2]
    step_cols = min(256, chunk)

    def project(index, first=False, c=None):
        def tile(j, carry):
            at = pl.ds(pl.multiple_of(j * step_cols, 128), step_cols)
            rows = pl.ds(pl.multiple_of(index * wide, 128), wide)
            value = jnp.dot(
                branch[:, column(index, wide)], proj_w[rows, at], preferred_element_type=jnp.float32
            )
            acc[:, at] = value if first else acc[:, at] + value
            return carry

        tiles = chunk // step_cols
        lo, hi = (0, chunks * tiles) if c is None else (c * tiles, (c + 1) * tiles)
        lax.fori_loop(lo, hi, tile, 0)

    def branch_arrived(index, sem, h):
        region = branch_region(index, h)
        return remote(region, region, sem, sem, (me, partner))

    project(t, True)
    for h in (1, 0):
        branch_arrived(partner, bp_recv.at[0, h], h).wait_recv()
    project(partner)
    for d in range(1, chips):
        source = chip_at(-d)
        for h in (1, 0):
            branch_arrived(source, by_recv.at[d, h], h).wait_recv()
            region = branch_region(source, h)
            copy = remote(region, region, bp_send.at[d, h], bp_recv.at[d, h], (me, partner))
            copy.start()
            sends.append(copy)
        project(source)
    for d in range(1, chips):
        source = chip_at(-d) + partner - t
        for h in (1, 0):
            branch_arrived(source, bp_recv.at[d, h], h).wait_recv()
        if d < chips - 1:
            project(source)

    guarded = []

    def token_region(index, c):
        if c == chunks:
            return early.at[index]
        return tokens.at[index, :, pl.ds(c * chunk, chunk)]

    def pass_on(index, c, sem, target):
        inside = (target >= 0) & (target < depth)
        copy = remote(
            token_region(index, c),
            token_region(index, c),
            sem,
            a_recv.at[index, c],
            (target * across + x, t),
        )

        @pl.when(inside)
        def _():
            copy.start()

        return inside, copy

    def share_scale():
        for d in range(1, tp):
            other = lax.rem(t + tp - d, tp)
            remote(
                squares.at[other], squares.at[other], s_send.at[d], s_recv.at[d], (me, other)
            ).wait_recv()
        total_sq = jnp.sum(squares[...], axis=0)
        scales[me] = lax.rsqrt(total_sq / (tp * cols) + EPS)
        for d in range(1, n):
            copy = remote(
                scales.at[me],
                scales.at[me],
                c_send.at[d],
                c_recv.at[me],
                (lax.rem(me + d, n), t),
            )
            copy.start()
            sends.append(copy)

    slot_rows = lax.broadcasted_iota(jnp.int32, (cap, row_count), 0).astype(jnp.float32)

    def wait_keys(origin):
        remote(
            key_rows.at[origin], key_rows.at[origin], k_send.at[1], k_recv.at[origin], (me, partner)
        ).wait_recv()

    def slot_scale(g, d):
        origin = group_z(g) * across + lax.rem(x + across - d, across)
        if d > 0:
            wait_keys(origin)
        if g > 0 or d > 0:
            remote(
                scales.at[origin], scales.at[origin], c_send.at[1], c_recv.at[origin], (me, partner)
            ).wait_recv()
        mine = slot_rows == key_rows[origin, pl.ds(me, 1), :]
        return jnp.sum(jnp.where(mine, scales[origin, 0:1, :], 0.0), axis=1, keepdims=True)

    def fan_region(f, index, c, late=False):
        lo = max(c * chunk, ahead_cols) if late else c * chunk
        hi = (c + 1) * chunk
        if c == chunks:
            lo, hi = 0, ahead_cols
        return piece.at[f, :, pl.ds(pl.multiple_of(index * cols + lo, 128), hi - lo)]

    def home(c):
        return chip_at(1) if c == chunks else t

    def select(g, c, far=True):
        source = group_z(g)
        origin = source * across + x
        peers = [z * across + lax.rem(x + d, across) for d in range(across)]
        at = pl.ds(0, ahead_cols) if c == chunks else pl.ds(c * chunk, chunk)
        buffer = early if c == chunks else tokens
        lo = cols if c == chunks else c * chunk
        width = ahead_cols if c == chunks else chunk
        slots = [
            slots_out.at[g, d - 1, :, pl.ds(lo, width)] for d in range(1, across)
        ]
        crossing = [
            remote(
                slots[d - 1],
                fan_region(g * across + d, home(c), c),
                x_send.at[g, d - 1, c],
                x_recv.at[g, d - 1, c],
                (peers[d], t),
            )
            for d in range(1, across)
        ]
        staying = fan_copies(g, 0, c)
        if far:
            sends.extend(crossing + staying)

        def body():
            if g > 0 and c == 0:
                wait_keys(origin)
            for d in list(range(1, across)) + [0]:
                chosen = jnp.where(
                    slot_rows == key_rows[origin, pl.ds(peers[d], 1), :], 1.0, 0.0
                ).astype(jnp.bfloat16)
                value = jnp.dot(
                    chosen, buffer[source, :, at], preferred_element_type=jnp.float32
                ).astype(jnp.bfloat16)
                if d == 0:
                    fan_region(g * across, home(c), c)[...] = value
                    for copy in staying if far else ():
                        copy.start()
                else:
                    slots[d - 1][...] = value
                    crossing[d - 1].start()

        return body

    def fan_copies(g, d, c):
        f = g * across + d
        region = fan_region(f, home(c), c)
        late = fan_region(f, t, c, True)
        copies = [
            remote(late, late, y_send.at[e, f, c], y_recv.at[e, f, c], (me, chip_at(e)))
            for e in range(1, chips if c < chunks else 1)
        ]
        copies.append(
            remote(region, region, p_send.at[0, f, c], p_recv.at[0, f, c], (me, partner))
        )
        return copies

    def fan_out(g, d, c):
        region = fan_region(g * across + d, home(c), c)
        remote(
            region, region, x_send.at[g, d - 1, c], x_recv.at[g, d - 1, c], (me, partner)
        ).wait_recv()
        for copy in fan_copies(g, d, c):
            copy.start()
            sends.append(copy)

    def arrive(step, c):
        for g in range(step, min(2 * step, depth - 1) + 1):
            source = group_z(g)
            due = jnp.abs(source - z) == step

            @pl.when(due)
            def _():
                remote(
                    token_region(source, c),
                    token_region(source, c),
                    a_send.at[g, c],
                    a_recv.at[source, c],
                    (me, partner),
                ).wait_recv()

            target = jnp.where(source < z, z + 1, z - 1)
            ahead = due & (target >= 0) & (target < depth)
            copy = remote(
                token_region(source, c),
                token_region(source, c),
                a_send.at[g, c],
                a_recv.at[source, c],
                (target * across + x, t),
            )

            @pl.when(ahead)
            def _():
                copy.start()

            guarded.append((ahead, copy))
        if step > 1:
            pl.when(jnp.logical_not(is_early(step)))(select(step, c))
        else:
            select(step, c)()

    def select_early(g):
        if 1 < g < depth:
            for c in range(pieces):
                pl.when(is_early(g))(select(g, c, False))

    def release(g):
        for c in range(pieces if 1 < g < depth else 0):
            for copy in fan_copies(g, 0, c):
                pl.when(is_early(g))(copy.start)

    def relay(g):
        for f in range(g * across, (g + 1) * across):
            for c in range(chunks):
                for d in range(1, chips):
                    region = fan_region(f, chip_at(-d), c, True)
                    remote(
                        region, region, y_send.at[d, f, c], y_recv.at[d, f, c], (me, partner)
                    ).wait_recv()
                    copy = remote(
                        region, region, p_send.at[d, f, c], p_recv.at[d, f, c], (me, partner)
                    )
                    copy.start()
                    sends.append(copy)

    def hid_region(g, index, h):
        return hid.at[
            g, :, pl.ds(pl.multiple_of(index * ffn_local + h * hid_step, 128), hid_step)
        ]

    def up_stage(g, send=True):
        for f in range(g * across, (g + 1) * across):
            for c in range(chunks):
                for d in range(chips):
                    region = fan_region(f, chip_at(-d) + partner - t, c, d > 0)
                    remote(
                        region, region, p_send.at[d, f, c], p_recv.at[d, f, c], (me, partner)
                    ).wait_recv()
            if ahead_cols:
                region = fan_region(f, chip_at(1) + partner - t, chunks)
                remote(
                    region, region, p_send.at[0, f, chunks], p_recv.at[0, f, chunks], (me, partner)
                ).wait_recv()
        if g == 0:
            weight_copies[0].wait()
            weight_copies[1].wait()
        scale = jnp.concatenate([slot_scale(g, d) for d in range(across)], axis=0)

        for h in range(ffn_local // hid_step):
            rows = piece[pl.ds(g * across, across)].reshape(group_rows, tp * cols)
            at = pl.ds(h * hid_step, hid_step)
            gate_val = jnp.dot(rows, gate_w[:, at], preferred_element_type=jnp.float32)
            up_val = jnp.dot(rows, up_w[:, at], preferred_element_type=jnp.float32)
            hidden = (jax.nn.silu(gate_val * scale) * (up_val * scale)).astype(jnp.bfloat16)
            hid[
                g, :, pl.ds(pl.multiple_of(t * ffn_local + h * hid_step, 128), hid_step)
            ] = hidden
            if send:
                send_hidden(g, h)

    def send_hidden(g, h):
        region = hid_region(g, t, h)
        for d in range(1, chips):
            copy = remote(
                region, region, hy_send.at[d, g, h], hy_recv.at[d, g, h], (me, chip_at(d))
            )
            copy.start()
            sends.append(copy)
        copy = remote(region, region, hp_send.at[0, g, h], hp_recv.at[0, g, h], (me, partner))
        copy.start()
        sends.append(copy)

    def relay_hidden(g):
        for h in range(ffn_local // hid_step):
            for d in range(1, chips):
                region = hid_region(g, chip_at(-d), h)
                remote(
                    region, region, hy_send.at[d, g, h], hy_recv.at[d, g, h], (me, partner)
                ).wait_recv()
                copy = remote(
                    region, region, hp_send.at[d, g, h], hp_recv.at[d, g, h], (me, partner)
                )
                copy.start()
                sends.append(copy)

    down_ready = []

    def down_stage(g):
        for h in range(ffn_local // hid_step):
            for d in range(chips):
                region = hid_region(g, chip_at(-d) + partner - t, h)
                remote(
                    region, region, hp_send.at[d, g, h], hp_recv.at[d, g, h], (me, partner)
                ).wait_recv()
        if not down_ready:
            weight_copies[2].wait()
            down_ready.append(g)
        step = min(256, cols)

        def tile(j, carry):
            at = pl.ds(pl.multiple_of(j * step, 128), step)
            value = jnp.dot(hid[g], down_w[:, at], preferred_element_type=jnp.float32)
            eo[pl.ds(g * across, across), :, at] = value.astype(jnp.bfloat16).reshape(
                across, cap, step
            )
            return carry

        lax.fori_loop(0, cols // step, tile, 0)

    def send_back(g, offsets):
        for d in offsets:
            if g == 0 and d == 0:
                continue
            k = g * across + d
            copy = remote(
                eo.at[k],
                ret_ref.at[me],
                r_send.at[k],
                r_recv.at[me],
                (group_z(g) * across + lax.rem(x + across - d, across), t),
            )
            copy.start()
            sends.append(copy)

    total[...] = jnp.zeros_like(total)

    def resid_tile(j, carry):
        at = pl.ds(pl.multiple_of(j * 128, 128), 128)
        value = (residual_ref[:, at].astype(jnp.float32) + acc[:, at]).astype(jnp.bfloat16)
        resid[:, at] = value
        value = value.astype(jnp.float32)
        total[...] += value * value
        tokens[z, :, at] = (value * gain_row[:, at]).astype(jnp.bfloat16)
        return carry

    early_copy = None
    for c in range(chunks):
        project(source, c=c)
        lax.fori_loop(c * chunk // 128, (c + 1) * chunk // 128, resid_tile, 0)
        if c == 0 and ahead_cols:
            early_copy = remote(
                tokens.at[z, :, pl.ds(0, ahead_cols)],
                early.at[z],
                e_send.at[0],
                e_recv.at[0],
                (me, chip_at(1)),
            )
            early_copy.start()
            sends.append(early_copy)
        guarded.append(pass_on(z, c, a_send.at[0, c], z + 1))
        guarded.append(pass_on(z, c, a_send.at[depth, c], z - 1))
        if c == chunks - 1:
            squares[t] = jnp.broadcast_to(
                jnp.sum(total[...].T, axis=0, keepdims=True), (8, row_count)
            )
            for d in range(1, tp):
                copy = remote(
                    squares.at[t],
                    squares.at[t],
                    s_send.at[d],
                    s_recv.at[d],
                    (me, lax.rem(t + d, tp)),
                )
                copy.start()
                sends.append(copy)
        select(0, c)()
    if ahead_cols:
        early_copy.wait_recv()
        guarded.append(pass_on(z, chunks, a_send.at[0, chunks], z + 1))
        guarded.append(pass_on(z, chunks, a_send.at[depth, chunks], z - 1))
        select(0, chunks)()

    def fan_across(g, c):
        for d in range(1, across):
            fan_out(g, d, c)

    for c in range(chunks):
        fan_across(0, c)
    share_scale()

    def up_part(g, send=True):
        relay(g)
        up_stage(g, send)

    def down_part(g, offsets=None):
        relay_hidden(g)
        down_stage(g)
        send_back(g, range(across) if offsets is None else offsets)

    for s in range(1, depth):
        arrive(s, 0)
        if s == 1:
            for c in range(chunks, pieces):
                fan_across(0, c)
            for c in range(1, pieces):
                arrive(s, c)
            select_early(s + 1)
            for c in range(pieces):
                fan_across(s, c)
            release(s + 1)
            up_part(0, False)
        elif s == 2:
            up_part(s - 1)
            for c in range(1, pieces):
                arrive(s, c)
            select_early(s + 1)
            for c in range(pieces):
                fan_across(s, c)
            release(s + 1)
        else:
            down_part(s - 2, [0])
            for c in range(1, chunks):
                arrive(s, c)
            up_part(s - 1)
            for c in range(chunks, pieces):
                arrive(s, c)
            send_back(s - 2, range(1, across))
            select_early(s + 1)
            for c in range(pieces):
                fan_across(s, c)
            release(s + 1)
    if last > 1:
        down_part(last - 1)
    up_part(last, last > 0)
    for h in range(ffn_local // hid_step):
        send_hidden(0, h)
    if last > 0:
        down_part(last)
    down_part(0)

    lanes = lax.broadcasted_iota(jnp.int32, (row_count, 128), 1)
    slot_lanes = lax.broadcasted_iota(jnp.int32, (row_count, cap), 1).astype(jnp.float32)
    turns = [*range(1, last), 0, last] if last > 0 else [0]
    for turn, g in enumerate(turns):
        chosen = []
        for d in range(across):
            there = group_z(g) * across + lax.rem(x + d, across)
            own = g == 0 and d == 0
            if not own:
                k = g * across + d
                remote(
                    eo.at[k], ret_ref.at[there], r_send.at[k], r_recv.at[there], (me, partner)
                ).wait_recv()
            here = lanes == there
            key = jnp.sum(jnp.where(here, key_col[...], 0.0), axis=1, keepdims=True)
            weight = jnp.sum(jnp.where(here, mix_col[...], 0.0), axis=1, keepdims=True)
            slot_of = jnp.where(slot_lanes == key, 1.0, 0.0).astype(jnp.bfloat16)
            chosen.append((eo.at[0] if own else ret_ref.at[there], slot_of, weight))
        step = min(256, cols)

        def combine(j, carry):
            at = pl.ds(pl.multiple_of(j * step, 128), step)
            value = jnp.zeros((row_count, step), jnp.float32) if turn == 0 else acc[:, at]
            for source, slot_of, weight in chosen:
                value = value + weight * jnp.dot(
                    slot_of, source[:, at], preferred_element_type=jnp.float32
                )
            if turn == depth - 1:
                result_ref[:, at] = (resid[:, at].astype(jnp.float32) + value).astype(jnp.bfloat16)
            else:
                acc[:, at] = value
            return carry

        lax.fori_loop(0, cols // step, combine, 0)
    for copy in sends:
        copy.wait_send()
    for started, copy in guarded:
        pl.when(started)(copy.wait_send)


def whole_layer(blocks, weights):
    n, tp = lax.axis_size("sp"), lax.axis_size("tp")
    row_count, wide = blocks[0].shape
    cols = blocks[5].shape[1]
    cap = 4 * row_count // n
    chips = tp // 2
    rows = n * cap
    across = max(d for d in range(1, n + 1) if n % d == 0 and d * d <= n)
    depth = n // across
    chunks = 2 if chips == 2 else 1
    ahead_cols = cols // 4 if chips == 2 else 0
    projection, gate_weight, _, down_weight = weights
    width, ffn_local = gate_weight.shape[1], gate_weight.shape[2]
    ffn = down_weight.shape[1]
    dma = pltpu.SemaphoreType.DMA
    bf16, f32 = jnp.bfloat16, jnp.float32
    parts = max(1, ffn_local // 256)
    flops = 2 * rows * width * ffn_local * 2 + 2 * rows * ffn * cols
    return pl.pallas_call(
        functools.partial(expert_kernel, n, tp, across),
        out_shape=jax.ShapeDtypeStruct((row_count, cols), bf16),
        in_specs=[pl.BlockSpec(memory_space=pltpu.VMEM)] * len(blocks)
        + [pl.BlockSpec(memory_space=pl.ANY)] * len(weights),
        out_specs=pl.BlockSpec(memory_space=pltpu.VMEM),
        scratch_shapes=[
            pltpu.VMEM((depth, row_count, cols), bf16),
            pltpu.VMEM((depth, row_count, ahead_cols or 128), bf16),
            pltpu.VMEM((depth, max(1, across - 1), cap, cols + ahead_cols), bf16),
            pltpu.VMEM((n, cap, cols), bf16),
            pltpu.VMEM((row_count, wide * tp), bf16),
            pltpu.VMEM(projection.shape, bf16),
            pltpu.VMEM((row_count, cols), f32),
            pltpu.VMEM((row_count, cols), bf16),
            pltpu.VMEM((tp, 8, row_count), f32),
            pltpu.VMEM((row_count, 128), f32),
            pltpu.VMEM((n, 8, row_count), f32),
            pltpu.VMEM((1, cols), f32),
            pltpu.VMEM((row_count, 128), f32),
            pltpu.VMEM((n, -(-n // 8) * 8, row_count), f32),
            pltpu.VMEM((row_count, 128), f32),
            pltpu.VMEM((8, row_count), f32),
            pltpu.VMEM((16, wide), bf16),
            pltpu.VMEM((16, wide), bf16),
            pltpu.VMEM((8, 128), f32),
            pltpu.VMEM((n, cap, width), bf16),
            pltpu.VMEM((depth, rows // depth, ffn), bf16),
            pltpu.VMEM((n, cap, cols), bf16),
            pltpu.VMEM((width, ffn_local), bf16),
            pltpu.VMEM((width, ffn_local), bf16),
            pltpu.VMEM((ffn, cols), bf16),
            dma((4,)),
            dma((n,)),
            dma((n,)),
            dma((n,)),
            dma((n,)),
            dma((2 if ahead_cols else 1,)),
            dma((1,)),
            dma((depth + 1, chunks + 1)),
            dma((depth, chunks + 1)),
            dma((depth, across, chunks + 1)),
            dma((depth, across, chunks + 1)),
            dma((chips, n, chunks + 1)),
            dma((chips, n, chunks + 1)),
            dma((chips, n, chunks + 1)),
            dma((chips, n, chunks + 1)),
            dma((chips, depth, parts)),
            dma((chips, depth, parts)),
            dma((chips, depth, parts)),
            dma((chips, depth, parts)),
            dma((n,)),
            dma((n,)),
            dma((3,)),
            dma((3,)),
            dma((chips, 2)),
            dma((chips, 2)),
            dma((chips, 2)),
            dma((chips, 2)),
            dma((tp,)),
            dma((tp,)),
        ],
        compiler_params=pltpu.CompilerParams(
            collective_id=0, has_side_effects=True, vmem_limit_bytes=56 * 1024 * 1024
        ),
        cost_estimate=pl.CostEstimate(
            flops=flops, bytes_accessed=3 * width * ffn_local * 2, transcendentals=0
        ),
        name="layer",
    )(*blocks, *weights)


def per_device(
    outer_gate,
    inner_gate,
    conv_input,
    conv_weight,
    doc_ids,
    output_weight,
    residual,
    norm_gain,
    expert_ids,
    group_weight,
    expert_weight,
    gate_weight,
    up_weight,
    down_weight,
):
    return whole_layer(
        (
            outer_gate,
            inner_gate,
            conv_input,
            conv_weight,
            doc_ids,
            residual,
            norm_gain,
            expert_ids.T,
            group_weight,
            expert_weight.T,
        ),
        (output_weight, gate_weight, up_weight, down_weight),
    )


def solution(mesh):
    return jax.shard_map(
        per_device,
        mesh=mesh,
        in_specs=(
            P("sp", "tp"),
            P("sp", "tp"),
            P("sp", "tp"),
            P(None, "tp"),
            P("sp"),
            P(None, "tp"),
            P("sp", "tp"),
            P("tp"),
            P("sp", None),
            P("sp"),
            P("sp", None),
            P("sp", None, "tp"),
            P("sp", None, "tp"),
            P("sp", None, "tp"),
        ),
        out_specs=P("sp", "tp"),
        check_vma=False,
    )
```

```python
import functools

import jax
import jax.numpy as jnp
from jax import lax
from jax.experimental import pallas as pl
from jax.experimental.pallas import tpu as pltpu
from jax.sharding import PartitionSpec as P

EPS = 1e-06
MESH = pl.DeviceIdType.MESH


def remote(src, dst, send_sem, recv_sem, device):
    return pltpu.make_async_remote_copy(
        src_ref=src,
        dst_ref=dst,
        send_sem=send_sem,
        recv_sem=recv_sem,
        device_id=device,
        device_id_type=MESH,
    )


def expert_kernel(
    n,
    tp,
    across,
    outer_ref,
    inner_ref,
    conv_ref,
    taps_ref,
    docs_ref,
    residual_ref,
    gain_ref,
    ids_ref,
    group_ref,
    mix_ref,
    proj_hbm,
    gate_hbm,
    up_hbm,
    down_hbm,
    result_ref,
    tokens,
    early,
    slots_out,
    ret_ref,
    branch,
    proj_w,
    acc,
    resid,
    squares,
    total,
    scales,
    gain_row,
    key_col,
    key_rows,
    mix_col,
    docs_rows,
    halo_inner,
    halo_conv,
    halo_docs,
    piece,
    hid,
    eo,
    gate_w,
    up_w,
    down_w,
    w_sem,
    k_send,
    k_recv,
    c_send,
    c_recv,
    e_send,
    e_recv,
    a_send,
    a_recv,
    x_send,
    x_recv,
    y_send,
    y_recv,
    p_send,
    p_recv,
    hy_send,
    hy_recv,
    hp_send,
    hp_recv,
    r_send,
    r_recv,
    h_send,
    h_recv,
    by_send,
    by_recv,
    bp_send,
    bp_recv,
    s_send,
    s_recv,
):
    me = lax.axis_index("sp")
    t = lax.axis_index("tp")
    chips = tp // 2
    y, core = lax.div(t, 2), lax.rem(t, 2)
    partner = t + 1 - 2 * core
    cap, cols = ret_ref.shape[1], ret_ref.shape[2]
    ffn_local = gate_w.shape[1]
    depth, group_rows = hid.shape[0], hid.shape[1]
    z, x = lax.div(me, across), lax.rem(me, across)
    ahead_cols = early.shape[2] if e_send.shape[0] > 1 else 0
    chunks = x_recv.shape[2] - 1
    last = depth - 1
    pieces = chunks + (1 if ahead_cols else 0)
    key_count = key_rows.shape[1]

    near = jnp.minimum(z, depth - 1 - z)
    low = 2 * z < depth

    def group_z(g):
        if g == 0:
            return z
        step = (g + 1) // 2
        outward = step if g % 2 else -step
        close = jnp.where(low, z + outward, z - outward)
        return jnp.where(g <= 2 * near, close, jnp.where(low, g, depth - 1 - g))

    def is_early(g):
        return jnp.abs(group_z(g) - z) < g

    def column(index, width):
        return pl.ds(pl.multiple_of(index * width, 128), width)

    def chip_at(delta):
        return lax.rem(y + delta + chips, chips) * 2 + core

    weight_copies = [
        pltpu.make_async_copy(source, target, w_sem.at[i])
        for i, (source, target) in enumerate(
            (
                (gate_hbm.at[0], gate_w),
                (up_hbm.at[0], up_w),
                (down_hbm.at[0], down_w),
                (proj_hbm, proj_w),
            )
        )
    ]
    for i in (3, 0, 1, 2):
        weight_copies[i].start()

    barrier = pltpu.get_barrier_semaphore()
    for k in range(1, n):
        pl.semaphore_signal(
            barrier, inc=1, device_id=(lax.rem(me + k, n), t), device_id_type=MESH
        )
    for d in range(1, tp):
        pl.semaphore_signal(
            barrier, inc=1, device_id=(me, lax.rem(t + d, tp)), device_id_type=MESH
        )

    sends = []
    row_count = residual_ref.shape[0]
    wide = branch.shape[1] // tp
    half = row_count // 2

    experts = lax.broadcasted_iota(jnp.int32, (128, row_count), 0)
    is_first, is_second = experts == ids_ref[0:1, :], experts == ids_ref[1:2, :]
    pair = mix_ref[...]
    mix = group_ref[...].reshape(1, row_count) * pair / (pair[0:1] + pair[1:2])
    mix_rows = jnp.where(is_first, mix[0:1], 0.0) + jnp.where(is_second, mix[1:2], 0.0)
    mix_col[...] = mix_rows.T
    member = jnp.where(is_first, 1.0, 0.0) + jnp.where(is_second, 1.0, 0.0)
    earlier = jnp.where(
        lax.broadcasted_iota(jnp.int32, (row_count, row_count), 0)
        < lax.broadcasted_iota(jnp.int32, (row_count, row_count), 1),
        1.0,
        0.0,
    ).astype(jnp.bfloat16)
    ranks = jnp.dot(member.astype(jnp.bfloat16), earlier, preferred_element_type=jnp.float32)
    keys = jnp.where(member > 0.5, ranks, -1.0)
    key_col[...] = keys.T
    key_rows[me] = keys[0:key_count]
    gain_row[...] = gain_ref[...].reshape(1, cols).astype(jnp.float32)

    docs = jnp.broadcast_to(docs_ref[...].reshape(1, row_count).astype(jnp.float32), (8, row_count))
    docs_rows[...] = docs
    position = lax.broadcasted_iota(jnp.int32, (8, row_count), 1)

    def as_column(mask):
        rows = jnp.where(mask, 1.0, 0.0)[0:1]
        return jnp.broadcast_to(rows, (128, rows.shape[1])).T > 0.5

    same_one = as_column((pltpu.roll(docs, 1, 1) == docs) & (position >= 1))
    same_two = as_column((pltpu.roll(docs, 2, 1) == docs) & (position >= 2))

    def weigh(at, products, one, two, first, second, outer):
        taps = taps_ref[:, at].astype(jnp.float32)
        conv = taps[2:3] * products
        conv = conv + jnp.where(first, taps[1:2] * one, 0.0)
        conv = conv + jnp.where(second, taps[0:1] * two, 0.0)
        return (outer.astype(jnp.float32) * conv).astype(jnp.bfloat16)

    def conv_tile(j, carry):
        at = pl.ds(pl.multiple_of(j * 128, 128), 128)
        products = inner_ref[:, at].astype(jnp.float32) * conv_ref[:, at].astype(jnp.float32)
        one, two = pltpu.roll(products, 1, 0), pltpu.roll(products, 2, 0)
        value = weigh(at, products, one, two, same_one, same_two, outer_ref[:, at])
        branch[:, pl.ds(pl.multiple_of(t * wide + j * 128, 128), 128)] = value
        return carry

    lax.fori_loop(0, wide // 128, conv_tile, 0)

    pl.semaphore_wait(barrier, n - 1 + tp - 1)

    halos = []
    following = (lax.rem(me + 1, n), t)
    for i, (source, target) in enumerate(
        (
            (inner_ref.at[pl.ds(row_count - 16, 16)], halo_inner),
            (conv_ref.at[pl.ds(row_count - 16, 16)], halo_conv),
            (docs_rows.at[:, pl.ds(row_count - 128, 128)], halo_docs),
        )
    ):
        copy = remote(source, target, h_send.at[i], h_recv.at[i], following)
        copy.start()
        halos.append(copy)
        sends.append(copy)

    def branch_region(index, h):
        return branch.at[pl.ds(h * half, half), column(index, wide)]

    def send_branch(h):
        region = branch_region(t, h)
        for d in range(1, chips):
            copy = remote(region, region, by_send.at[d - 1, h], by_recv.at[d - 1, h], (me, chip_at(d)))
            copy.start()
            sends.append(copy)
        copy = remote(region, region, bp_send.at[0, h], bp_recv.at[0, h], (me, partner))
        copy.start()
        sends.append(copy)

    send_branch(1)
    for d in range(1, n):
        copy = remote(
            key_rows.at[me],
            key_rows.at[me],
            k_send.at[d],
            k_recv.at[me],
            (lax.rem(me + d, n), t),
        )
        copy.start()
        sends.append(copy)

    for copy in halos:
        copy.wait_recv()
    lane = lax.broadcasted_iota(jnp.int32, (8, 128), 1)
    near_docs = docs_rows[:, 0:128]
    past_docs = jnp.where(me > 0, halo_docs[...], -1.0)
    docs_one = jnp.where(lane < 1, pltpu.roll(past_docs, 1, 1), pltpu.roll(near_docs, 1, 1))
    docs_two = jnp.where(lane < 2, pltpu.roll(past_docs, 2, 1), pltpu.roll(near_docs, 2, 1))
    edge_one = as_column(docs_one == near_docs)[0:16]
    edge_two = as_column(docs_two == near_docs)[0:16]
    row_at = lax.broadcasted_iota(jnp.int32, (16, 1), 0)
    for j in range(wide // 128):
        at = pl.ds(j * 128, 128)
        products = inner_ref[0:16, at].astype(jnp.float32) * conv_ref[0:16, at].astype(jnp.float32)
        before = halo_inner[:, at].astype(jnp.float32) * halo_conv[:, at].astype(jnp.float32)
        one = jnp.where(row_at < 1, pltpu.roll(before, 1, 0), pltpu.roll(products, 1, 0))
        two = jnp.where(row_at < 2, pltpu.roll(before, 2, 0), pltpu.roll(products, 2, 0))
        value = weigh(at, products, one, two, edge_one, edge_two, outer_ref[0:16, at])
        branch[0:16, pl.ds(pl.multiple_of(t * wide + j * 128, 128), 128)] = value
    send_branch(0)
    weight_copies[3].wait()

    chunk = cols // chunks
    hid_step = ffn_local // hy_send.shape[2]
    step_cols = min(256, chunk)

    def project(index, first=False, c=None):
        def tile(j, carry):
            at = pl.ds(pl.multiple_of(j * step_cols, 128), step_cols)
            rows = pl.ds(pl.multiple_of(index * wide, 128), wide)
            value = jnp.dot(
                branch[:, column(index, wide)], proj_w[rows, at], preferred_element_type=jnp.float32
            )
            acc[:, at] = value if first else acc[:, at] + value
            return carry

        tiles = chunk // step_cols
        lo, hi = (0, chunks * tiles) if c is None else (c * tiles, (c + 1) * tiles)
        lax.fori_loop(lo, hi, tile, 0)

    def branch_arrived(index, sem, h):
        region = branch_region(index, h)
        return remote(region, region, sem, sem, (me, partner))

    project(t, True)
    for h in (1, 0):
        branch_arrived(partner, bp_recv.at[0, h], h).wait_recv()
    project(partner)
    for d in range(1, chips):
        source = chip_at(-d)
        for h in (1, 0):
            branch_arrived(source, by_recv.at[d - 1, h], h).wait_recv()
            region = branch_region(source, h)
            copy = remote(region, region, bp_send.at[d, h], bp_recv.at[d, h], (me, partner))
            copy.start()
            sends.append(copy)
        project(source)
    for d in range(1, chips):
        source = chip_at(-d) + partner - t
        for h in (1, 0):
            branch_arrived(source, bp_recv.at[d, h], h).wait_recv()
        if d < chips - 1:
            project(source)

    guarded = []

    def token_region(index, c):
        if c == chunks:
            return early.at[index]
        return tokens.at[index, :, pl.ds(c * chunk, chunk)]

    def pass_on(index, c, sem, target):
        inside = (target >= 0) & (target < depth)
        copy = remote(
            token_region(index, c),
            token_region(index, c),
            sem,
            a_recv.at[index, c],
            (target * across + x, t),
        )

        @pl.when(inside)
        def _():
            copy.start()

        return inside, copy

    def share_scale():
        for d in range(1, tp):
            other = lax.rem(t + tp - d, tp)
            remote(
                squares.at[other], squares.at[other], s_send.at[d], s_recv.at[d], (me, other)
            ).wait_recv()
        total_sq = jnp.sum(squares[...], axis=0)
        scales[me] = lax.rsqrt(total_sq / (tp * cols) + EPS)
        for d in range(1, n):
            copy = remote(
                scales.at[me],
                scales.at[me],
                c_send.at[d],
                c_recv.at[me],
                (lax.rem(me + d, n), t),
            )
            copy.start()
            sends.append(copy)

    slot_rows = lax.broadcasted_iota(jnp.int32, (cap, row_count), 0).astype(jnp.float32)

    def wait_keys(origin):
        remote(
            key_rows.at[origin], key_rows.at[origin], k_send.at[1], k_recv.at[origin], (me, partner)
        ).wait_recv()

    def slot_scale(g, d):
        origin = group_z(g) * across + lax.rem(x + across - d, across)
        if d > 0:
            wait_keys(origin)
        if g > 0 or d > 0:
            remote(
                scales.at[origin], scales.at[origin], c_send.at[1], c_recv.at[origin], (me, partner)
            ).wait_recv()
        mine = slot_rows == key_rows[origin, pl.ds(me, 1), :]
        return jnp.sum(jnp.where(mine, scales[origin, 0:1, :], 0.0), axis=1, keepdims=True)

    def fan_region(f, index, c, late=False):
        lo = max(c * chunk, ahead_cols) if late else c * chunk
        hi = (c + 1) * chunk
        if c == chunks:
            lo, hi = 0, ahead_cols
        return piece.at[f, :, pl.ds(pl.multiple_of(index * cols + lo, 128), hi - lo)]

    def home(c):
        return chip_at(1) if c == chunks else t

    def select(g, c, far=True):
        source = group_z(g)
        origin = source * across + x
        peers = [z * across + lax.rem(x + d, across) for d in range(across)]
        at = pl.ds(0, ahead_cols) if c == chunks else pl.ds(c * chunk, chunk)
        buffer = early if c == chunks else tokens
        lo = cols if c == chunks else c * chunk
        width = ahead_cols if c == chunks else chunk
        slots = [
            slots_out.at[g, d - 1, :, pl.ds(lo, width)] for d in range(1, across)
        ]
        crossing = [
            remote(
                slots[d - 1],
                fan_region(g * across + d, home(c), c),
                x_send.at[g, d - 1, c],
                x_recv.at[g, d - 1, c],
                (peers[d], t),
            )
            for d in range(1, across)
        ]
        staying = fan_copies(g, 0, c)
        if far:
            sends.extend(crossing + staying)

        def body():
            if g > 0 and c == 0:
                wait_keys(origin)
            for d in list(range(1, across)) + [0]:
                chosen = jnp.where(
                    slot_rows == key_rows[origin, pl.ds(peers[d], 1), :], 1.0, 0.0
                ).astype(jnp.bfloat16)
                value = jnp.dot(
                    chosen, buffer[source, :, at], preferred_element_type=jnp.float32
                ).astype(jnp.bfloat16)
                if d == 0:
                    fan_region(g * across, home(c), c)[...] = value
                    for copy in staying if far else ():
                        copy.start()
                else:
                    slots[d - 1][...] = value
                    crossing[d - 1].start()

        return body

    def fan_copies(g, d, c):
        f = g * across + d
        region = fan_region(f, home(c), c)
        late = fan_region(f, t, c, True)
        copies = [
            remote(late, late, y_send.at[e - 1, f, c], y_recv.at[e - 1, f, c], (me, chip_at(e)))
            for e in range(1, chips if c < chunks else 1)
        ]
        copies.append(
            remote(region, region, p_send.at[0, f, c], p_recv.at[0, f, c], (me, partner))
        )
        return copies

    def fan_out(g, d, c):
        region = fan_region(g * across + d, home(c), c)
        remote(
            region, region, x_send.at[g, d - 1, c], x_recv.at[g, d - 1, c], (me, partner)
        ).wait_recv()
        for copy in fan_copies(g, d, c):
            copy.start()

    def arrive(step, c):
        for g in range(step, min(2 * step, depth - 1) + 1):
            source = group_z(g)
            due = jnp.abs(source - z) == step

            @pl.when(due)
            def _():
                remote(
                    token_region(source, c),
                    token_region(source, c),
                    a_send.at[g, c],
                    a_recv.at[source, c],
                    (me, partner),
                ).wait_recv()

            target = jnp.where(source < z, z + 1, z - 1)
            ahead = due & (target >= 0) & (target < depth)
            copy = remote(
                token_region(source, c),
                token_region(source, c),
                a_send.at[g, c],
                a_recv.at[source, c],
                (target * across + x, t),
            )

            @pl.when(ahead)
            def _():
                copy.start()

            guarded.append((ahead, copy))
        if step > 1:
            pl.when(jnp.logical_not(is_early(step)))(select(step, c))
        else:
            select(step, c)()

    def select_early(g):
        if 1 < g < depth:
            for c in range(pieces):
                pl.when(is_early(g))(select(g, c, False))

    def release(g):
        for c in range(pieces if 1 < g < depth else 0):
            for copy in fan_copies(g, 0, c):
                pl.when(is_early(g))(copy.start)

    def relay_pairs(g):
        pairs = []
        for f in range(g * across, (g + 1) * across):
            for c in range(chunks):
                for d in range(1, chips):
                    region = fan_region(f, chip_at(-d), c, True)
                    pairs.append(
                        (
                            remote(
                                region,
                                region,
                                y_send.at[d - 1, f, c],
                                y_recv.at[d - 1, f, c],
                                (me, partner),
                            ),
                            remote(
                                region,
                                region,
                                p_send.at[d, f, c],
                                p_recv.at[d, f, c],
                                (me, partner),
                            ),
                        )
                    )
        return pairs

    def relay(g):
        for arrival, copy in relay_pairs(g):
            arrival.wait_recv()
            copy.start()

    def hid_region(g, index, h):
        return hid.at[
            g, :, pl.ds(pl.multiple_of(index * ffn_local + h * hid_step, 128), hid_step)
        ]

    def up_stage(g, send=True):
        for f in range(g * across, (g + 1) * across):
            for c in range(chunks):
                for d in range(chips):
                    region = fan_region(f, chip_at(-d) + partner - t, c, d > 0)
                    remote(
                        region, region, p_send.at[d, f, c], p_recv.at[d, f, c], (me, partner)
                    ).wait_recv()
            if ahead_cols:
                region = fan_region(f, chip_at(1) + partner - t, chunks)
                remote(
                    region, region, p_send.at[0, f, chunks], p_recv.at[0, f, chunks], (me, partner)
                ).wait_recv()
        if g == 0:
            weight_copies[0].wait()
            weight_copies[1].wait()
        scale = jnp.concatenate([slot_scale(g, d) for d in range(across)], axis=0)

        for h in range(ffn_local // hid_step):
            rows = piece[pl.ds(g * across, across)].reshape(group_rows, tp * cols)
            at = pl.ds(h * hid_step, hid_step)
            gate_val = jnp.dot(rows, gate_w[:, at], preferred_element_type=jnp.float32)
            up_val = jnp.dot(rows, up_w[:, at], preferred_element_type=jnp.float32)
            hidden = (jax.nn.silu(gate_val * scale) * (up_val * scale)).astype(jnp.bfloat16)
            hid[
                g, :, pl.ds(pl.multiple_of(t * ffn_local + h * hid_step, 128), hid_step)
            ] = hidden
            if send:
                send_hidden(g, h)

    def hidden_copies(g, h):
        region = hid_region(g, t, h)
        copies = [
            remote(region, region, hy_send.at[d - 1, g, h], hy_recv.at[d - 1, g, h], (me, chip_at(d)))
            for d in range(1, chips)
        ]
        copies.append(
            remote(region, region, hp_send.at[0, g, h], hp_recv.at[0, g, h], (me, partner))
        )
        return copies

    def send_hidden(g, h):
        for copy in hidden_copies(g, h):
            copy.start()

    def relay_hidden(g):
        for h in range(ffn_local // hid_step):
            for d in range(1, chips):
                region = hid_region(g, chip_at(-d), h)
                remote(
                    region, region, hy_send.at[d - 1, g, h], hy_recv.at[d - 1, g, h], (me, partner)
                ).wait_recv()
                copy = remote(
                    region, region, hp_send.at[d, g, h], hp_recv.at[d, g, h], (me, partner)
                )
                copy.start()
                sends.append(copy)

    down_ready = []
    returns = []

    def down_stage(g):
        for h in range(ffn_local // hid_step):
            for d in range(chips):
                region = hid_region(g, chip_at(-d) + partner - t, h)
                remote(
                    region, region, hp_send.at[d, g, h], hp_recv.at[d, g, h], (me, partner)
                ).wait_recv()
        if not down_ready:
            weight_copies[2].wait()
            down_ready.append(g)
        step = min(256, cols)

        def tile(j, carry):
            at = pl.ds(pl.multiple_of(j * step, 128), step)
            value = jnp.dot(hid[g], down_w[:, at], preferred_element_type=jnp.float32)
            eo[pl.ds(g * across, across), :, at] = value.astype(jnp.bfloat16).reshape(
                across, cap, step
            )
            return carry

        lax.fori_loop(0, cols // step, tile, 0)

    def send_back(g, offsets):
        for d in offsets:
            if g == 0 and d == 0:
                continue
            k = g * across + d
            copy = remote(
                eo.at[k],
                ret_ref.at[me],
                r_send.at[k],
                r_recv.at[me],
                (group_z(g) * across + lax.rem(x + across - d, across), t),
            )
            copy.start()
            returns.append(copy)

    total[...] = jnp.zeros_like(total)

    def resid_tile(j, carry):
        at = pl.ds(pl.multiple_of(j * 128, 128), 128)
        value = (residual_ref[:, at].astype(jnp.float32) + acc[:, at]).astype(jnp.bfloat16)
        resid[:, at] = value
        value = value.astype(jnp.float32)
        total[...] += value * value
        tokens[z, :, at] = (value * gain_row[:, at]).astype(jnp.bfloat16)
        return carry

    early_copy = None
    for c in range(chunks):
        project(source, c=c)
        lax.fori_loop(c * chunk // 128, (c + 1) * chunk // 128, resid_tile, 0)
        if c == 0 and ahead_cols:
            early_copy = remote(
                tokens.at[z, :, pl.ds(0, ahead_cols)],
                early.at[z],
                e_send.at[0],
                e_recv.at[0],
                (me, chip_at(1)),
            )
            early_copy.start()
            sends.append(early_copy)
        guarded.append(pass_on(z, c, a_send.at[0, c], z + 1))
        guarded.append(pass_on(z, c, a_send.at[depth, c], z - 1))
        if c == chunks - 1:
            squares[t] = jnp.broadcast_to(
                jnp.sum(total[...].T, axis=0, keepdims=True), (8, row_count)
            )
            for d in range(1, tp):
                copy = remote(
                    squares.at[t],
                    squares.at[t],
                    s_send.at[d],
                    s_recv.at[d],
                    (me, lax.rem(t + d, tp)),
                )
                copy.start()
                sends.append(copy)
        select(0, c)()
    if ahead_cols:
        early_copy.wait_recv()
        guarded.append(pass_on(z, chunks, a_send.at[0, chunks], z + 1))
        guarded.append(pass_on(z, chunks, a_send.at[depth, chunks], z - 1))
        select(0, chunks)()

    def fan_across(g, c):
        for d in range(1, across):
            fan_out(g, d, c)

    for c in range(chunks):
        fan_across(0, c)
    share_scale()

    def up_part(g, send=True):
        relay(g)
        up_stage(g, send)

    def down_part(g, offsets=None):
        relay_hidden(g)
        down_stage(g)
        send_back(g, range(across) if offsets is None else offsets)

    def when_early(g, then, work):
        if 1 < g:
            early_here = is_early(g)
            pl.when(early_here if then else jnp.logical_not(early_here))(work)
        elif not then:
            work()

    for s in range(1, depth):
        arrive(s, 0)
        if s == 1:
            for c in range(chunks, pieces):
                fan_across(0, c)
            for c in range(1, pieces):
                arrive(s, c)
            select_early(s + 1)
            for c in range(pieces):
                fan_across(s, c)
            release(s + 1)
            up_part(0, False)
        elif s == 2:
            up_part(s - 1)
            for c in range(1, pieces):
                arrive(s, c)
            select_early(s + 1)
            for c in range(pieces):
                fan_across(s, c)
            release(s + 1)
        else:
            down_part(s - 2, [0])
            for c in range(pieces):
                when_early(s, True, functools.partial(fan_across, s, c))
            for c in range(1, chunks):
                arrive(s, c)
            up_part(s - 1)
            for c in range(chunks, pieces):
                arrive(s, c)
            send_back(s - 2, range(1, across))
            select_early(s + 1)
            for c in range(pieces):
                when_early(s, False, functools.partial(fan_across, s, c))
            release(s + 1)
    when_early(last, True, functools.partial(up_part, last, last > 0))
    if last > 1:
        down_part(last - 1)
    when_early(last, False, functools.partial(up_part, last, last > 0))
    for h in range(ffn_local // hid_step):
        send_hidden(0, h)
    if last > 0:
        down_part(last)
    down_part(0)

    for copy in sends:
        copy.wait_send()
    for started, copy in guarded:
        pl.when(started)(copy.wait_send)
    for g in range(depth):
        for _, copy in relay_pairs(g):
            copy.wait_send()
        for h in range(ffn_local // hid_step):
            for copy in hidden_copies(g, h):
                copy.wait_send()
        for d in range(1, across):
            for c in range(pieces):
                for copy in fan_copies(g, d, c):
                    copy.wait_send()

    lanes = lax.broadcasted_iota(jnp.int32, (row_count, 128), 1)
    slot_lanes = lax.broadcasted_iota(jnp.int32, (row_count, cap), 1).astype(jnp.float32)
    turns = [*range(1, last - 1), last, last - 1, 0] if last > 1 else [*range(last, -1, -1)]
    for turn, g in enumerate(turns):
        chosen = []
        for d in range(across):
            there = group_z(g) * across + lax.rem(x + d, across)
            own = g == 0 and d == 0
            if not own:
                k = g * across + d
                remote(
                    eo.at[k], ret_ref.at[there], r_send.at[k], r_recv.at[there], (me, partner)
                ).wait_recv()
            here = lanes == there
            key = jnp.sum(jnp.where(here, key_col[...], 0.0), axis=1, keepdims=True)
            weight = jnp.sum(jnp.where(here, mix_col[...], 0.0), axis=1, keepdims=True)
            slot_of = jnp.where(slot_lanes == key, 1.0, 0.0).astype(jnp.bfloat16)
            chosen.append((eo.at[0] if own else ret_ref.at[there], slot_of, weight))
        step = min(256, cols)

        def combine(j, carry):
            at = pl.ds(pl.multiple_of(j * step, 128), step)
            value = jnp.zeros((row_count, step), jnp.float32) if turn == 0 else acc[:, at]
            for source, slot_of, weight in chosen:
                value = value + weight * jnp.dot(
                    slot_of, source[:, at], preferred_element_type=jnp.float32
                )
            if turn == depth - 1:
                result_ref[:, at] = (resid[:, at].astype(jnp.float32) + value).astype(jnp.bfloat16)
            else:
                acc[:, at] = value
            return carry

        lax.fori_loop(0, cols // step, combine, 0)
    for copy in returns:
        copy.wait_send()


def whole_layer(blocks, weights):
    n, tp = lax.axis_size("sp"), lax.axis_size("tp")
    row_count, wide = blocks[0].shape
    cols = blocks[5].shape[1]
    cap = 4 * row_count // n
    chips = tp // 2
    rows = n * cap
    across = max(d for d in range(1, n + 1) if n % d == 0 and d * d <= n)
    depth = n // across
    chunks = 2 if chips == 2 else 1
    ahead_cols = cols // 4 if chips == 2 else 0
    projection, gate_weight, _, down_weight = weights
    width, ffn_local = gate_weight.shape[1], gate_weight.shape[2]
    ffn = down_weight.shape[1]
    dma = pltpu.SemaphoreType.DMA
    bf16, f32 = jnp.bfloat16, jnp.float32
    parts = max(1, ffn_local // 256)
    flops = 2 * rows * width * ffn_local * 2 + 2 * rows * ffn * cols
    return pl.pallas_call(
        functools.partial(expert_kernel, n, tp, across),
        out_shape=jax.ShapeDtypeStruct((row_count, cols), bf16),
        in_specs=[pl.BlockSpec(memory_space=pltpu.VMEM)] * len(blocks)
        + [pl.BlockSpec(memory_space=pl.ANY)] * len(weights),
        out_specs=pl.BlockSpec(memory_space=pltpu.VMEM),
        scratch_shapes=[
            pltpu.VMEM((depth, row_count, cols), bf16),
            pltpu.VMEM((depth, row_count, ahead_cols or 128), bf16),
            pltpu.VMEM((depth, max(1, across - 1), cap, cols + ahead_cols), bf16),
            pltpu.VMEM((n, cap, cols), bf16),
            pltpu.VMEM((row_count, wide * tp), bf16),
            pltpu.VMEM(projection.shape, bf16),
            pltpu.VMEM((row_count, cols), f32),
            pltpu.VMEM((row_count, cols), bf16),
            pltpu.VMEM((tp, 8, row_count), f32),
            pltpu.VMEM((row_count, 128), f32),
            pltpu.VMEM((n, 8, row_count), f32),
            pltpu.VMEM((1, cols), f32),
            pltpu.VMEM((row_count, 128), f32),
            pltpu.VMEM((n, -(-n // 8) * 8, row_count), f32),
            pltpu.VMEM((row_count, 128), f32),
            pltpu.VMEM((8, row_count), f32),
            pltpu.VMEM((16, wide), bf16),
            pltpu.VMEM((16, wide), bf16),
            pltpu.VMEM((8, 128), f32),
            pltpu.VMEM((n, cap, width), bf16),
            pltpu.VMEM((depth, rows // depth, ffn), bf16),
            pltpu.VMEM((n, cap, cols), bf16),
            pltpu.VMEM((width, ffn_local), bf16),
            pltpu.VMEM((width, ffn_local), bf16),
            pltpu.VMEM((ffn, cols), bf16),
            dma((4,)),
            dma((n,)),
            dma((n,)),
            dma((n,)),
            dma((n,)),
            dma((2 if ahead_cols else 1,)),
            dma((1,)),
            dma((depth + 1, chunks + 1)),
            dma((depth, chunks + 1)),
            dma((depth, max(1, across - 1), chunks + 1)),
            dma((depth, max(1, across - 1), chunks + 1)),
            dma((max(1, chips - 1), n, chunks)),
            dma((max(1, chips - 1), n, chunks)),
            dma((chips, n, chunks + 1)),
            dma((chips, n, chunks + 1)),
            dma((max(1, chips - 1), depth, parts)),
            dma((max(1, chips - 1), depth, parts)),
            dma((chips, depth, parts)),
            dma((chips, depth, parts)),
            dma((n,)),
            dma((n,)),
            dma((3,)),
            dma((3,)),
            dma((max(1, chips - 1), 2)),
            dma((max(1, chips - 1), 2)),
            dma((chips, 2)),
            dma((chips, 2)),
            dma((tp,)),
            dma((tp,)),
        ],
        compiler_params=pltpu.CompilerParams(
            collective_id=0, has_side_effects=True, vmem_limit_bytes=56 * 1024 * 1024
        ),
        cost_estimate=pl.CostEstimate(
            flops=flops, bytes_accessed=3 * width * ffn_local * 2, transcendentals=0
        ),
        name="layer",
    )(*blocks, *weights)


def per_device(
    outer_gate,
    inner_gate,
    conv_input,
    conv_weight,
    doc_ids,
    output_weight,
    residual,
    norm_gain,
    expert_ids,
    group_weight,
    expert_weight,
    gate_weight,
    up_weight,
    down_weight,
):
    return whole_layer(
        (
            outer_gate,
            inner_gate,
            conv_input,
            conv_weight,
            doc_ids,
            residual,
            norm_gain,
            expert_ids.T,
            group_weight,
            expert_weight.T,
        ),
        (output_weight, gate_weight, up_weight, down_weight),
    )


def solution(mesh):
    return jax.shard_map(
        per_device,
        mesh=mesh,
        in_specs=(
            P("sp", "tp"),
            P("sp", "tp"),
            P("sp", "tp"),
            P(None, "tp"),
            P("sp"),
            P(None, "tp"),
            P("sp", "tp"),
            P("tp"),
            P("sp", None),
            P("sp"),
            P("sp", None),
            P("sp", None, "tp"),
            P("sp", None, "tp"),
            P("sp", None, "tp"),
        ),
        out_specs=P("sp", "tp"),
        check_vma=False,
    )
```

```python
import functools

import jax
import jax.numpy as jnp
from jax import lax
from jax.experimental import pallas as pl
from jax.experimental.pallas import tpu as pltpu
from jax.sharding import PartitionSpec as P

EPS = 1e-06
MESH = pl.DeviceIdType.MESH


def remote(src, dst, send_sem, recv_sem, device):
    return pltpu.make_async_remote_copy(
        src_ref=src,
        dst_ref=dst,
        send_sem=send_sem,
        recv_sem=recv_sem,
        device_id=device,
        device_id_type=MESH,
    )


def expert_kernel(
    n,
    tp,
    across,
    outer_ref,
    inner_ref,
    conv_ref,
    taps_ref,
    docs_ref,
    residual_ref,
    gain_ref,
    ids_ref,
    group_ref,
    mix_ref,
    proj_hbm,
    gate_hbm,
    up_hbm,
    down_hbm,
    result_ref,
    tokens,
    early,
    slots_out,
    ret_ref,
    branch,
    proj_w,
    acc,
    resid,
    squares,
    total,
    scales,
    gain_row,
    key_col,
    key_rows,
    mix_col,
    docs_rows,
    halo_inner,
    halo_conv,
    halo_docs,
    piece,
    hid,
    eo,
    gate_w,
    up_w,
    down_w,
    w_sem,
    k_send,
    k_recv,
    c_send,
    c_recv,
    e_send,
    e_recv,
    a_send,
    a_recv,
    x_send,
    x_recv,
    y_send,
    y_recv,
    p_send,
    p_recv,
    hy_send,
    hy_recv,
    hp_send,
    hp_recv,
    r_send,
    r_recv,
    h_send,
    h_recv,
    by_send,
    by_recv,
    bp_send,
    bp_recv,
    s_send,
    s_recv,
):
    me = lax.axis_index("sp")
    t = lax.axis_index("tp")
    chips = tp // 2
    y, core = lax.div(t, 2), lax.rem(t, 2)
    partner = t + 1 - 2 * core
    cap, cols = ret_ref.shape[1], ret_ref.shape[2]
    ffn_local = gate_w.shape[1]
    depth, group_rows = hid.shape[0], hid.shape[1]
    z, x = lax.div(me, across), lax.rem(me, across)
    ahead_cols = early.shape[2] if e_send.shape[0] > 1 else 0
    chunks = x_recv.shape[2] - 1
    last = depth - 1
    pieces = chunks + (1 if ahead_cols else 0)
    key_count = key_rows.shape[1]

    near = jnp.minimum(z, depth - 1 - z)
    low = 2 * z < depth

    def group_z(g):
        if g == 0:
            return z
        step = (g + 1) // 2
        outward = step if g % 2 else -step
        close = jnp.where(low, z + outward, z - outward)
        return jnp.where(g <= 2 * near, close, jnp.where(low, g, depth - 1 - g))

    def is_early(g):
        return jnp.abs(group_z(g) - z) < g

    def column(index, width):
        return pl.ds(pl.multiple_of(index * width, 128), width)

    def chip_at(delta):
        return lax.rem(y + delta + chips, chips) * 2 + core

    weight_copies = [
        pltpu.make_async_copy(source, target, w_sem.at[i])
        for i, (source, target) in enumerate(
            (
                (gate_hbm.at[0], gate_w),
                (up_hbm.at[0], up_w),
                (down_hbm.at[0], down_w),
                (proj_hbm, proj_w),
            )
        )
    ]
    for i in (3, 0, 1, 2):
        weight_copies[i].start()

    barrier = pltpu.get_barrier_semaphore()
    for k in range(1, n):
        pl.semaphore_signal(
            barrier, inc=1, device_id=(lax.rem(me + k, n), t), device_id_type=MESH
        )
    for d in range(1, tp):
        pl.semaphore_signal(
            barrier, inc=1, device_id=(me, lax.rem(t + d, tp)), device_id_type=MESH
        )

    sends = []
    row_count = residual_ref.shape[0]
    wide = branch.shape[1] // tp
    half = row_count // 2

    experts = lax.broadcasted_iota(jnp.int32, (128, row_count), 0)
    is_first, is_second = experts == ids_ref[0:1, :], experts == ids_ref[1:2, :]
    pair = mix_ref[...]
    mix = group_ref[...].reshape(1, row_count) * pair / (pair[0:1] + pair[1:2])
    mix_rows = jnp.where(is_first, mix[0:1], 0.0) + jnp.where(is_second, mix[1:2], 0.0)
    mix_col[...] = mix_rows.T
    member = jnp.where(is_first, 1.0, 0.0) + jnp.where(is_second, 1.0, 0.0)
    earlier = jnp.where(
        lax.broadcasted_iota(jnp.int32, (row_count, row_count), 0)
        < lax.broadcasted_iota(jnp.int32, (row_count, row_count), 1),
        1.0,
        0.0,
    ).astype(jnp.bfloat16)
    ranks = jnp.dot(member.astype(jnp.bfloat16), earlier, preferred_element_type=jnp.float32)
    keys = jnp.where(member > 0.5, ranks, -1.0)
    key_col[...] = keys.T
    key_rows[me] = keys[0:key_count]
    gain_row[...] = gain_ref[...].reshape(1, cols).astype(jnp.float32)

    docs = jnp.broadcast_to(docs_ref[...].reshape(1, row_count).astype(jnp.float32), (8, row_count))
    docs_rows[...] = docs
    position = lax.broadcasted_iota(jnp.int32, (8, row_count), 1)

    def as_column(mask):
        rows = jnp.where(mask, 1.0, 0.0)[0:1]
        return jnp.broadcast_to(rows, (128, rows.shape[1])).T > 0.5

    same_one = as_column((pltpu.roll(docs, 1, 1) == docs) & (position >= 1))
    same_two = as_column((pltpu.roll(docs, 2, 1) == docs) & (position >= 2))

    def weigh(at, products, one, two, first, second, outer):
        taps = taps_ref[:, at].astype(jnp.float32)
        conv = taps[2:3] * products
        conv = conv + jnp.where(first, taps[1:2] * one, 0.0)
        conv = conv + jnp.where(second, taps[0:1] * two, 0.0)
        return (outer.astype(jnp.float32) * conv).astype(jnp.bfloat16)

    def conv_tile(j, carry):
        at = pl.ds(pl.multiple_of(j * 128, 128), 128)
        products = inner_ref[:, at].astype(jnp.float32) * conv_ref[:, at].astype(jnp.float32)
        one, two = pltpu.roll(products, 1, 0), pltpu.roll(products, 2, 0)
        value = weigh(at, products, one, two, same_one, same_two, outer_ref[:, at])
        branch[:, pl.ds(pl.multiple_of(t * wide + j * 128, 128), 128)] = value
        return carry

    lax.fori_loop(0, wide // 128, conv_tile, 0)

    pl.semaphore_wait(barrier, n - 1 + tp - 1)

    halos = []
    following = (lax.rem(me + 1, n), t)
    for i, (source, target) in enumerate(
        (
            (inner_ref.at[pl.ds(row_count - 16, 16)], halo_inner),
            (conv_ref.at[pl.ds(row_count - 16, 16)], halo_conv),
            (docs_rows.at[:, pl.ds(row_count - 128, 128)], halo_docs),
        )
    ):
        copy = remote(source, target, h_send.at[i], h_recv.at[i], following)
        copy.start()
        halos.append(copy)
        sends.append(copy)

    def branch_region(index, h):
        return branch.at[pl.ds(h * half, half), column(index, wide)]

    def send_branch(h):
        region = branch_region(t, h)
        for d in range(1, chips):
            copy = remote(region, region, by_send.at[d - 1, h], by_recv.at[d - 1, h], (me, chip_at(d)))
            copy.start()
            sends.append(copy)
        copy = remote(region, region, bp_send.at[0, h], bp_recv.at[0, h], (me, partner))
        copy.start()
        sends.append(copy)

    send_branch(1)
    for d in range(1, n):
        copy = remote(
            key_rows.at[me],
            key_rows.at[me],
            k_send.at[d],
            k_recv.at[me],
            (lax.rem(me + d, n), t),
        )
        copy.start()
        sends.append(copy)

    for copy in halos:
        copy.wait_recv()
    lane = lax.broadcasted_iota(jnp.int32, (8, 128), 1)
    near_docs = docs_rows[:, 0:128]
    past_docs = jnp.where(me > 0, halo_docs[...], -1.0)
    docs_one = jnp.where(lane < 1, pltpu.roll(past_docs, 1, 1), pltpu.roll(near_docs, 1, 1))
    docs_two = jnp.where(lane < 2, pltpu.roll(past_docs, 2, 1), pltpu.roll(near_docs, 2, 1))
    edge_one = as_column(docs_one == near_docs)[0:16]
    edge_two = as_column(docs_two == near_docs)[0:16]
    row_at = lax.broadcasted_iota(jnp.int32, (16, 1), 0)
    for j in range(wide // 128):
        at = pl.ds(j * 128, 128)
        products = inner_ref[0:16, at].astype(jnp.float32) * conv_ref[0:16, at].astype(jnp.float32)
        before = halo_inner[:, at].astype(jnp.float32) * halo_conv[:, at].astype(jnp.float32)
        one = jnp.where(row_at < 1, pltpu.roll(before, 1, 0), pltpu.roll(products, 1, 0))
        two = jnp.where(row_at < 2, pltpu.roll(before, 2, 0), pltpu.roll(products, 2, 0))
        value = weigh(at, products, one, two, edge_one, edge_two, outer_ref[0:16, at])
        branch[0:16, pl.ds(pl.multiple_of(t * wide + j * 128, 128), 128)] = value
    send_branch(0)
    weight_copies[3].wait()

    chunk = cols // chunks
    hid_step = ffn_local // hy_send.shape[2]
    step_cols = min(256, chunk)

    def project(index, first=False, c=None):
        def tile(j, carry):
            at = pl.ds(pl.multiple_of(j * step_cols, 128), step_cols)
            rows = pl.ds(pl.multiple_of(index * wide, 128), wide)
            value = jnp.dot(
                branch[:, column(index, wide)], proj_w[rows, at], preferred_element_type=jnp.float32
            )
            acc[:, at] = value if first else acc[:, at] + value
            return carry

        tiles = chunk // step_cols
        lo, hi = (0, chunks * tiles) if c is None else (c * tiles, (c + 1) * tiles)
        lax.fori_loop(lo, hi, tile, 0)

    def branch_arrived(index, sem, h):
        region = branch_region(index, h)
        return remote(region, region, sem, sem, (me, partner))

    project(t, True)
    for h in (1, 0):
        branch_arrived(partner, bp_recv.at[0, h], h).wait_recv()
    project(partner)
    for d in range(1, chips):
        source = chip_at(-d)
        for h in (1, 0):
            branch_arrived(source, by_recv.at[d - 1, h], h).wait_recv()
            region = branch_region(source, h)
            copy = remote(region, region, bp_send.at[d, h], bp_recv.at[d, h], (me, partner))
            copy.start()
            sends.append(copy)
        project(source)
    for d in range(1, chips):
        source = chip_at(-d) + partner - t
        for h in (1, 0):
            branch_arrived(source, bp_recv.at[d, h], h).wait_recv()
        if d < chips - 1:
            project(source)

    guarded = []

    def token_region(index, c):
        if c == chunks:
            return early.at[index]
        return tokens.at[index, :, pl.ds(c * chunk, chunk)]

    def pass_on(index, c, sem, target):
        inside = (target >= 0) & (target < depth)
        copy = remote(
            token_region(index, c),
            token_region(index, c),
            sem,
            a_recv.at[index, c],
            (target * across + x, t),
        )

        @pl.when(inside)
        def _():
            copy.start()

        return inside, copy

    def share_scale():
        for d in range(1, tp):
            other = lax.rem(t + tp - d, tp)
            remote(
                squares.at[other], squares.at[other], s_send.at[d], s_recv.at[d], (me, other)
            ).wait_recv()
        total_sq = jnp.sum(squares[...], axis=0)
        scales[me] = lax.rsqrt(total_sq / (tp * cols) + EPS)
        for d in range(1, n):
            copy = remote(
                scales.at[me],
                scales.at[me],
                c_send.at[d],
                c_recv.at[me],
                (lax.rem(me + d, n), t),
            )
            copy.start()
            sends.append(copy)

    slot_rows = lax.broadcasted_iota(jnp.int32, (cap, row_count), 0).astype(jnp.float32)

    def wait_keys(origin):
        remote(
            key_rows.at[origin], key_rows.at[origin], k_send.at[1], k_recv.at[origin], (me, partner)
        ).wait_recv()

    def slot_scale(g, d):
        origin = group_z(g) * across + lax.rem(x + across - d, across)
        if d > 0:
            wait_keys(origin)
        if g > 0 or d > 0:
            remote(
                scales.at[origin], scales.at[origin], c_send.at[1], c_recv.at[origin], (me, partner)
            ).wait_recv()
        mine = slot_rows == key_rows[origin, pl.ds(me, 1), :]
        return jnp.sum(jnp.where(mine, scales[origin, 0:1, :], 0.0), axis=1, keepdims=True)

    def fan_region(f, index, c, late=False):
        lo = max(c * chunk, ahead_cols) if late else c * chunk
        hi = (c + 1) * chunk
        if c == chunks:
            lo, hi = 0, ahead_cols
        return piece.at[f, :, pl.ds(pl.multiple_of(index * cols + lo, 128), hi - lo)]

    def home(c):
        return chip_at(1) if c == chunks else t

    def select(g, c, far=True):
        source = group_z(g)
        origin = source * across + x
        peers = [z * across + lax.rem(x + d, across) for d in range(across)]
        at = pl.ds(0, ahead_cols) if c == chunks else pl.ds(c * chunk, chunk)
        buffer = early if c == chunks else tokens
        lo = cols if c == chunks else c * chunk
        width = ahead_cols if c == chunks else chunk
        slots = [
            slots_out.at[g, d - 1, :, pl.ds(lo, width)] for d in range(1, across)
        ]
        crossing = [
            remote(
                slots[d - 1],
                fan_region(g * across + d, home(c), c),
                x_send.at[g, d - 1, c],
                x_recv.at[g, d - 1, c],
                (peers[d], t),
            )
            for d in range(1, across)
        ]
        staying = fan_copies(g, 0, c)
        if far:
            sends.extend(crossing + staying)

        def body():
            if g > 0 and c == 0:
                wait_keys(origin)
            for d in list(range(1, across)) + [0]:
                chosen = jnp.where(
                    slot_rows == key_rows[origin, pl.ds(peers[d], 1), :], 1.0, 0.0
                ).astype(jnp.bfloat16)
                value = jnp.dot(
                    chosen, buffer[source, :, at], preferred_element_type=jnp.float32
                ).astype(jnp.bfloat16)
                if d == 0:
                    fan_region(g * across, home(c), c)[...] = value
                    for copy in staying if far else ():
                        copy.start()
                else:
                    slots[d - 1][...] = value
                    crossing[d - 1].start()

        return body

    def fan_copies(g, d, c):
        f = g * across + d
        region = fan_region(f, home(c), c)
        late = fan_region(f, t, c, True)
        copies = [
            remote(late, late, y_send.at[e - 1, f, c], y_recv.at[e - 1, f, c], (me, chip_at(e)))
            for e in range(1, chips if c < chunks else 1)
        ]
        copies.append(
            remote(region, region, p_send.at[0, f, c], p_recv.at[0, f, c], (me, partner))
        )
        return copies

    def fan_out(g, d, c):
        region = fan_region(g * across + d, home(c), c)
        remote(
            region, region, x_send.at[g, d - 1, c], x_recv.at[g, d - 1, c], (me, partner)
        ).wait_recv()
        for copy in fan_copies(g, d, c):
            copy.start()

    def arrive(step, c):
        for g in range(step, min(2 * step, depth - 1) + 1):
            source = group_z(g)
            due = jnp.abs(source - z) == step

            @pl.when(due)
            def _():
                remote(
                    token_region(source, c),
                    token_region(source, c),
                    a_send.at[g, c],
                    a_recv.at[source, c],
                    (me, partner),
                ).wait_recv()

            target = jnp.where(source < z, z + 1, z - 1)
            ahead = due & (target >= 0) & (target < depth)
            copy = remote(
                token_region(source, c),
                token_region(source, c),
                a_send.at[g, c],
                a_recv.at[source, c],
                (target * across + x, t),
            )

            @pl.when(ahead)
            def _():
                copy.start()

            guarded.append((ahead, copy))
        if step > 1:
            pl.when(jnp.logical_not(is_early(step)))(select(step, c))
        else:
            select(step, c)()

    def select_early(g):
        if 1 < g < depth:
            for c in range(pieces):
                pl.when(is_early(g))(select(g, c, False))

    def release(g):
        for c in range(pieces if 1 < g < depth else 0):
            for copy in fan_copies(g, 0, c):
                pl.when(is_early(g))(copy.start)

    def relay_pairs(g):
        pairs = []
        for f in range(g * across, (g + 1) * across):
            for c in range(chunks):
                for d in range(1, chips):
                    region = fan_region(f, chip_at(-d), c, True)
                    pairs.append(
                        (
                            remote(
                                region,
                                region,
                                y_send.at[d - 1, f, c],
                                y_recv.at[d - 1, f, c],
                                (me, partner),
                            ),
                            remote(
                                region,
                                region,
                                p_send.at[d, f, c],
                                p_recv.at[d, f, c],
                                (me, partner),
                            ),
                        )
                    )
        return pairs

    def relay(g):
        for arrival, copy in relay_pairs(g):
            arrival.wait_recv()
            copy.start()

    def hid_region(g, index, h):
        return hid.at[
            g, :, pl.ds(pl.multiple_of(index * ffn_local + h * hid_step, 128), hid_step)
        ]

    def up_stage(g, send=True):
        for f in range(g * across, (g + 1) * across):
            for c in range(chunks):
                for d in range(chips):
                    region = fan_region(f, chip_at(-d) + partner - t, c, d > 0)
                    remote(
                        region, region, p_send.at[d, f, c], p_recv.at[d, f, c], (me, partner)
                    ).wait_recv()
            if ahead_cols:
                region = fan_region(f, chip_at(1) + partner - t, chunks)
                remote(
                    region, region, p_send.at[0, f, chunks], p_recv.at[0, f, chunks], (me, partner)
                ).wait_recv()
        if g == 0:
            weight_copies[0].wait()
            weight_copies[1].wait()
        scale = jnp.concatenate([slot_scale(g, d) for d in range(across)], axis=0)

        for h in range(ffn_local // hid_step):
            rows = piece[pl.ds(g * across, across)].reshape(group_rows, tp * cols)
            at = pl.ds(h * hid_step, hid_step)
            gate_val = jnp.dot(rows, gate_w[:, at], preferred_element_type=jnp.float32)
            up_val = jnp.dot(rows, up_w[:, at], preferred_element_type=jnp.float32)
            hidden = (jax.nn.silu(gate_val * scale) * (up_val * scale)).astype(jnp.bfloat16)
            hid[
                g, :, pl.ds(pl.multiple_of(t * ffn_local + h * hid_step, 128), hid_step)
            ] = hidden
            if send:
                send_hidden(g, h)

    def hidden_copies(g, h):
        region = hid_region(g, t, h)
        copies = [
            remote(region, region, hy_send.at[d - 1, g, h], hy_recv.at[d - 1, g, h], (me, chip_at(d)))
            for d in range(1, chips)
        ]
        copies.append(
            remote(region, region, hp_send.at[0, g, h], hp_recv.at[0, g, h], (me, partner))
        )
        return copies

    def send_hidden(g, h):
        for copy in hidden_copies(g, h):
            copy.start()

    def relay_hidden(g):
        for h in range(ffn_local // hid_step):
            for d in range(1, chips):
                region = hid_region(g, chip_at(-d), h)
                remote(
                    region, region, hy_send.at[d - 1, g, h], hy_recv.at[d - 1, g, h], (me, partner)
                ).wait_recv()
                copy = remote(
                    region, region, hp_send.at[d, g, h], hp_recv.at[d, g, h], (me, partner)
                )
                copy.start()
                sends.append(copy)

    down_ready = []
    returns = []

    def down_stage(g):
        for h in range(ffn_local // hid_step):
            for d in range(chips):
                region = hid_region(g, chip_at(-d) + partner - t, h)
                remote(
                    region, region, hp_send.at[d, g, h], hp_recv.at[d, g, h], (me, partner)
                ).wait_recv()
        if not down_ready:
            weight_copies[2].wait()
            down_ready.append(g)
        step = min(256, cols)

        def tile(j, carry):
            at = pl.ds(pl.multiple_of(j * step, 128), step)
            value = jnp.dot(hid[g], down_w[:, at], preferred_element_type=jnp.float32)
            eo[pl.ds(g * across, across), :, at] = value.astype(jnp.bfloat16).reshape(
                across, cap, step
            )
            return carry

        lax.fori_loop(0, cols // step, tile, 0)

    def send_back(g, offsets):
        for d in reversed(offsets):
            if g == 0 and d == 0:
                continue
            k = g * across + d
            copy = remote(
                eo.at[k],
                ret_ref.at[me],
                r_send.at[k],
                r_recv.at[me],
                (group_z(g) * across + lax.rem(x + across - d, across), t),
            )
            copy.start()
            returns.append(copy)

    total[...] = jnp.zeros_like(total)

    def resid_tile(j, carry):
        at = pl.ds(pl.multiple_of(j * 128, 128), 128)
        value = (residual_ref[:, at].astype(jnp.float32) + acc[:, at]).astype(jnp.bfloat16)
        resid[:, at] = value
        value = value.astype(jnp.float32)
        total[...] += value * value
        tokens[z, :, at] = (value * gain_row[:, at]).astype(jnp.bfloat16)
        return carry

    early_copy = None
    for c in range(chunks):
        project(source, c=c)
        lax.fori_loop(c * chunk // 128, (c + 1) * chunk // 128, resid_tile, 0)
        if c == 0 and ahead_cols:
            early_copy = remote(
                tokens.at[z, :, pl.ds(0, ahead_cols)],
                early.at[z],
                e_send.at[0],
                e_recv.at[0],
                (me, chip_at(1)),
            )
            early_copy.start()
            sends.append(early_copy)
        guarded.append(pass_on(z, c, a_send.at[0, c], z + 1))
        guarded.append(pass_on(z, c, a_send.at[depth, c], z - 1))
        if c == chunks - 1:
            squares[t] = jnp.broadcast_to(
                jnp.sum(total[...].T, axis=0, keepdims=True), (8, row_count)
            )
            for d in range(1, tp):
                copy = remote(
                    squares.at[t],
                    squares.at[t],
                    s_send.at[d],
                    s_recv.at[d],
                    (me, lax.rem(t + d, tp)),
                )
                copy.start()
                sends.append(copy)
        select(0, c)()
    if ahead_cols:
        early_copy.wait_recv()
        guarded.append(pass_on(z, chunks, a_send.at[0, chunks], z + 1))
        guarded.append(pass_on(z, chunks, a_send.at[depth, chunks], z - 1))
        select(0, chunks)()

    def fan_across(g, c):
        for d in range(1, across):
            fan_out(g, d, c)

    for c in range(chunks):
        fan_across(0, c)
    share_scale()

    def up_part(g, send=True):
        relay(g)
        up_stage(g, send)

    def down_part(g, offsets=None):
        relay_hidden(g)
        down_stage(g)
        send_back(g, range(across) if offsets is None else offsets)

    def when_early(g, then, work):
        if 1 < g:
            early_here = is_early(g)
            pl.when(early_here if then else jnp.logical_not(early_here))(work)
        elif not then:
            work()

    for s in range(1, depth):
        arrive(s, 0)
        if s == 1:
            for c in range(chunks, pieces):
                fan_across(0, c)
            for c in range(1, pieces):
                arrive(s, c)
            select_early(s + 1)
            for c in range(pieces):
                fan_across(s, c)
            release(s + 1)
            up_part(0, False)
        elif s == 2:
            up_part(s - 1)
            for c in range(1, pieces):
                arrive(s, c)
            select_early(s + 1)
            for c in range(pieces):
                fan_across(s, c)
            release(s + 1)
        else:
            down_part(s - 2, [0])
            for c in range(pieces):
                when_early(s, True, functools.partial(fan_across, s, c))
            for c in range(1, chunks):
                arrive(s, c)
            up_part(s - 1)
            for c in range(chunks, pieces):
                arrive(s, c)
            send_back(s - 2, range(1, across))
            select_early(s + 1)
            for c in range(pieces):
                when_early(s, False, functools.partial(fan_across, s, c))
            release(s + 1)
    when_early(last, True, functools.partial(up_part, last, last > 0))
    if last > 1:
        down_part(last - 1)
    when_early(last, False, functools.partial(up_part, last, last > 0))
    for h in range(ffn_local // hid_step):
        send_hidden(0, h)
    if last > 0:
        down_part(last)
    down_part(0)

    for copy in sends:
        copy.wait_send()
    for started, copy in guarded:
        pl.when(started)(copy.wait_send)
    for g in range(depth):
        for _, copy in relay_pairs(g):
            copy.wait_send()
        for h in range(ffn_local // hid_step):
            for copy in hidden_copies(g, h):
                copy.wait_send()
        for d in range(1, across):
            for c in range(pieces):
                for copy in fan_copies(g, d, c):
                    copy.wait_send()

    lanes = lax.broadcasted_iota(jnp.int32, (row_count, 128), 1)
    slot_lanes = lax.broadcasted_iota(jnp.int32, (row_count, cap), 1).astype(jnp.float32)
    turns = [*range(1, last - 1), last, last - 1, 0] if last > 1 else [*range(last, -1, -1)]
    for turn, g in enumerate(turns):
        chosen = []
        for d in range(across):
            there = group_z(g) * across + lax.rem(x + d, across)
            own = g == 0 and d == 0
            if not own:
                k = g * across + d
                remote(
                    eo.at[k], ret_ref.at[there], r_send.at[k], r_recv.at[there], (me, partner)
                ).wait_recv()
            here = lanes == there
            key = jnp.sum(jnp.where(here, key_col[...], 0.0), axis=1, keepdims=True)
            weight = jnp.sum(jnp.where(here, mix_col[...], 0.0), axis=1, keepdims=True)
            slot_of = jnp.where(slot_lanes == key, 1.0, 0.0).astype(jnp.bfloat16)
            chosen.append((eo.at[0] if own else ret_ref.at[there], slot_of, weight))
        step = min(256, cols)

        def combine(j, carry):
            at = pl.ds(pl.multiple_of(j * step, 128), step)
            value = jnp.zeros((row_count, step), jnp.float32) if turn == 0 else acc[:, at]
            for source, slot_of, weight in chosen:
                value = value + weight * jnp.dot(
                    slot_of, source[:, at], preferred_element_type=jnp.float32
                )
            if turn == depth - 1:
                result_ref[:, at] = (resid[:, at].astype(jnp.float32) + value).astype(jnp.bfloat16)
            else:
                acc[:, at] = value
            return carry

        lax.fori_loop(0, cols // step, combine, 0)
    for copy in returns:
        copy.wait_send()


def whole_layer(blocks, weights):
    n, tp = lax.axis_size("sp"), lax.axis_size("tp")
    row_count, wide = blocks[0].shape
    cols = blocks[5].shape[1]
    cap = 4 * row_count // n
    chips = tp // 2
    rows = n * cap
    across = max(d for d in range(1, n + 1) if n % d == 0 and d * d <= n)
    depth = n // across
    chunks = 2 if chips == 2 else 1
    ahead_cols = cols // 4 if chips == 2 else 0
    projection, gate_weight, _, down_weight = weights
    width, ffn_local = gate_weight.shape[1], gate_weight.shape[2]
    ffn = down_weight.shape[1]
    dma = pltpu.SemaphoreType.DMA
    bf16, f32 = jnp.bfloat16, jnp.float32
    parts = max(1, ffn_local // 256)
    flops = 2 * rows * width * ffn_local * 2 + 2 * rows * ffn * cols
    return pl.pallas_call(
        functools.partial(expert_kernel, n, tp, across),
        out_shape=jax.ShapeDtypeStruct((row_count, cols), bf16),
        in_specs=[pl.BlockSpec(memory_space=pltpu.VMEM)] * len(blocks)
        + [pl.BlockSpec(memory_space=pl.ANY)] * len(weights),
        out_specs=pl.BlockSpec(memory_space=pltpu.VMEM),
        scratch_shapes=[
            pltpu.VMEM((depth, row_count, cols), bf16),
            pltpu.VMEM((depth, row_count, ahead_cols or 128), bf16),
            pltpu.VMEM((depth, max(1, across - 1), cap, cols + ahead_cols), bf16),
            pltpu.VMEM((n, cap, cols), bf16),
            pltpu.VMEM((row_count, wide * tp), bf16),
            pltpu.VMEM(projection.shape, bf16),
            pltpu.VMEM((row_count, cols), f32),
            pltpu.VMEM((row_count, cols), bf16),
            pltpu.VMEM((tp, 8, row_count), f32),
            pltpu.VMEM((row_count, 128), f32),
            pltpu.VMEM((n, 8, row_count), f32),
            pltpu.VMEM((1, cols), f32),
            pltpu.VMEM((row_count, 128), f32),
            pltpu.VMEM((n, -(-n // 8) * 8, row_count), f32),
            pltpu.VMEM((row_count, 128), f32),
            pltpu.VMEM((8, row_count), f32),
            pltpu.VMEM((16, wide), bf16),
            pltpu.VMEM((16, wide), bf16),
            pltpu.VMEM((8, 128), f32),
            pltpu.VMEM((n, cap, width), bf16),
            pltpu.VMEM((depth, rows // depth, ffn), bf16),
            pltpu.VMEM((n, cap, cols), bf16),
            pltpu.VMEM((width, ffn_local), bf16),
            pltpu.VMEM((width, ffn_local), bf16),
            pltpu.VMEM((ffn, cols), bf16),
            dma((4,)),
            dma((n,)),
            dma((n,)),
            dma((n,)),
            dma((n,)),
            dma((2 if ahead_cols else 1,)),
            dma((1,)),
            dma((depth + 1, chunks + 1)),
            dma((depth, chunks + 1)),
            dma((depth, max(1, across - 1), chunks + 1)),
            dma((depth, max(1, across - 1), chunks + 1)),
            dma((max(1, chips - 1), n, chunks)),
            dma((max(1, chips - 1), n, chunks)),
            dma((chips, n, chunks + 1)),
            dma((chips, n, chunks + 1)),
            dma((max(1, chips - 1), depth, parts)),
            dma((max(1, chips - 1), depth, parts)),
            dma((chips, depth, parts)),
            dma((chips, depth, parts)),
            dma((n,)),
            dma((n,)),
            dma((3,)),
            dma((3,)),
            dma((max(1, chips - 1), 2)),
            dma((max(1, chips - 1), 2)),
            dma((chips, 2)),
            dma((chips, 2)),
            dma((tp,)),
            dma((tp,)),
        ],
        compiler_params=pltpu.CompilerParams(
            collective_id=0, has_side_effects=True, vmem_limit_bytes=56 * 1024 * 1024
        ),
        cost_estimate=pl.CostEstimate(
            flops=flops, bytes_accessed=3 * width * ffn_local * 2, transcendentals=0
        ),
        name="layer",
    )(*blocks, *weights)


def per_device(
    outer_gate,
    inner_gate,
    conv_input,
    conv_weight,
    doc_ids,
    output_weight,
    residual,
    norm_gain,
    expert_ids,
    group_weight,
    expert_weight,
    gate_weight,
    up_weight,
    down_weight,
):
    return whole_layer(
        (
            outer_gate,
            inner_gate,
            conv_input,
            conv_weight,
            doc_ids,
            residual,
            norm_gain,
            expert_ids.T,
            group_weight,
            expert_weight.T,
        ),
        (output_weight, gate_weight, up_weight, down_weight),
    )


def solution(mesh):
    return jax.shard_map(
        per_device,
        mesh=mesh,
        in_specs=(
            P("sp", "tp"),
            P("sp", "tp"),
            P("sp", "tp"),
            P(None, "tp"),
            P("sp"),
            P(None, "tp"),
            P("sp", "tp"),
            P("tp"),
            P("sp", None),
            P("sp"),
            P("sp", None),
            P("sp", None, "tp"),
            P("sp", None, "tp"),
            P("sp", None, "tp"),
        ),
        out_specs=P("sp", "tp"),
        check_vma=False,
    )
```
